32 devices in a mesh: sp: 8 (over z, y), tp: 4 (over x, core).
Axes of the slice: x: 2, y: 2, z: 4, core: 2. Of those that a mesh axis runs over, the one named last changes fastest.
Arguments:
- query: bfloat16 [4096, 1024], P('sp', 'tp'), may hold values from -6 to 6
- key: bfloat16 [4096, 1024], P('sp', 'tp'), may hold values from -6 to 6
- value: bfloat16 [4096, 1024], P('sp', 'tp'), may hold values from -6 to 6
- out_grad: bfloat16 [4096, 1024], P('sp', 'tp'), may hold values from -6 to 6
- query_gain: float32 [64], replicated, may hold values from 0.1 to 1.9
- key_gain: float32 [64], replicated, may hold values from 0.1 to 1.9
- rel_bias: float32 [16, 129], P('tp'), may hold values from -3 to 3
Outputs:
- query_grad: bfloat16 [4096, 1024], P('sp', 'tp')
- key_grad: bfloat16 [4096, 1024], P('sp', 'tp')
- value_grad: bfloat16 [4096, 1024], P('sp', 'tp')
- query_gain_grad: float32 [64], replicated
- key_gain_grad: float32 [64], replicated
- bias_grad: float32 [16, 129], P('tp')
The draws below stay inside these ranges and needn't reach their ends.
All inputs are finite; a program needn't handle non-finite values.
Results may differ from the reference program's by a relative error of at most 0.0095.
Values may be sent and summed in bfloat16 or wider, within the bound.
No kernel may reach another device: no remote copies, remote signals or barrier semaphores. Data moves between devices by JAX's collectives and lax.ppermute only.
A program may use at most 64 MiB of HBM per device.

```python
import jax
import jax.numpy as jnp
from jax import lax

H = 16
HD = 64
SEG = 64
PREV = 8
CLIP = 128
TOKENS = 4096
ATT = 1024
TAPS = 129


def block_levels(stream_key, extent, shards, smallest, top_value):
    loudness = 1.0
    for dim, blocks in shards:
        heights = jax.random.uniform(jax.random.fold_in(jax.random.fold_in(stream_key, 6), dim), (blocks,), jnp.float32, smallest / len(shards), top_value / len(shards))
        loudness = loudness * jnp.repeat(jnp.exp(heights), extent[dim] // blocks).reshape((-1,) + (1,) * (len(extent) - 1 - dim))
    return loudness


def noise(key, shape, scale, bound, pieces=(), kind=jnp.bfloat16):
    gain = block_levels(key, shape, pieces, -0.22, 0.18) if pieces else 1.0
    entries = jax.random.normal(key, shape, jnp.float32) * scale * gain
    return jnp.minimum(jnp.maximum(entries, -bound), bound).astype(kind)


def setup_inputs(seed: int = 0) -> dict:
    splits = jax.random.split(jax.random.key(seed), 8)
    return {
        "query": noise(splits[0], (TOKENS, ATT), 1.0, 6.0, ((0, 8), (1, 4))),
        "key": noise(splits[1], (TOKENS, ATT), 1.0, 6.0, ((0, 8), (1, 4))),
        "value": noise(splits[2], (TOKENS, ATT), 1.0, 6.0, ((0, 8), (1, 4))),
        "out_grad": noise(splits[3], (TOKENS, ATT), 1.0, 6.0, ((0, 8), (1, 4))),
        "query_gain": jnp.clip(1.0 + 0.18 * jax.random.normal(splits[4], (HD,), jnp.float32), 0.1, 1.9),
        "key_gain": jnp.clip(1.0 + 0.18 * jax.random.normal(splits[5], (HD,), jnp.float32), 0.1, 1.9),
        "rel_bias": noise(splits[6], (H, TAPS), 0.5, 3.0, ((0, 4),), jnp.float32),
    }


epsilon = 1e-06

def normalize(head_rows, gain_vector):
    widened = head_rows.astype(jnp.float32)
    row_scale = lax.rsqrt(lax.optimization_barrier(jnp.mean(widened * widened, axis=-1, keepdims=True)) + epsilon)
    unit_rows = widened * row_scale
    return (unit_rows, row_scale, (unit_rows * gain_vector).astype(jnp.bfloat16))

def norm_backward(grad_hat, unit_rows, row_scale, gain_vector):
    grad_unit = grad_hat * gain_vector
    inner_mean = lax.optimization_barrier(jnp.mean(grad_unit * unit_rows, axis=-1, keepdims=True))
    return (row_scale * (grad_unit - unit_rows * inner_mean), lax.optimization_barrier(jnp.sum(grad_hat * unit_rows, axis=(0, 1))))

def bias_matrix(table_row, block):
    tap_count = table_row.shape[0]
    position = jnp.arange(3 * block - 1, dtype=jnp.int32)
    distance = jnp.clip(2 * block - 1 - position, 0, tap_count - 1)
    selected = distance[:, None] == jnp.arange(tap_count, dtype=jnp.int32)[None, :]
    diagonal = lax.optimization_barrier(jnp.sum(jnp.where(selected, table_row[None, :], jnp.zeros((), table_row.dtype)), axis=1))
    diagonal = jnp.concatenate([diagonal[block - 1:], jnp.zeros((1,), diagonal.dtype), diagonal[:block - 1]])
    flattened = jnp.tile(diagonal, block)[:block * (3 * block - 1)]
    return flattened.reshape(block, 3 * block - 1)[:, :2 * block]

def tap_totals(score_grad, tap_count):
    block = score_grad.shape[0]
    widened = jnp.pad(score_grad, ((0, 0), (0, block - 1)))
    flattened = jnp.pad(widened.reshape(-1), (0, block))
    columns = lax.optimization_barrier(jnp.sum(flattened.reshape(block, 3 * block), axis=0))
    near_taps = columns[block - tap_count + 2:block + 1][::-1]
    return jnp.concatenate([near_taps, (jnp.sum(columns) - jnp.sum(near_taps))[None]])

def band_mask(block):
    row_index = jnp.arange(block, dtype=jnp.int32)[:, None]
    col_index = jnp.arange(2 * block, dtype=jnp.int32)[None, :]
    return (row_index + block >= col_index) & (col_index // SEG >= row_index // SEG)

def block_gradients(query_block, key_block, value_block, grad_block, bias_block, allowed, score_scale, skip_rows):
    scores = jnp.dot(query_block, key_block.T, preferred_element_type=jnp.float32) * score_scale + bias_block
    normalizer = lax.optimization_barrier(jnp.sum(jnp.where(allowed, jnp.exp(scores), jnp.zeros((), jnp.float32)), axis=1, keepdims=True))
    log_total = jnp.log(normalizer)
    attention = jnp.where(allowed, jnp.exp(scores - log_total), jnp.zeros((), jnp.float32))
    attention_low = attention.astype(jnp.bfloat16)
    output_low = jnp.dot(attention_low, value_block, preferred_element_type=jnp.float32).astype(jnp.bfloat16)
    output_low = lax.optimization_barrier(output_low)
    row_delta = lax.optimization_barrier(jnp.sum(grad_block.astype(jnp.float32) * output_low.astype(jnp.float32), axis=1, keepdims=True))
    attention_grad = jnp.dot(grad_block, value_block.T, preferred_element_type=jnp.float32)
    score_grad = attention * (attention_grad - row_delta)
    score_low = score_grad.astype(jnp.bfloat16)
    query_part = jnp.dot(score_low, key_block, preferred_element_type=jnp.float32) * score_scale
    key_part = jnp.dot(score_low[:, skip_rows:].T, query_block, preferred_element_type=jnp.float32) * score_scale
    value_part = jnp.dot(attention_low[:, skip_rows:].T, grad_block, preferred_element_type=jnp.float32)
    tap_part = tap_totals(score_grad, bias_block.shape[0] * 0 + CLIP + 1)
    return (query_part, key_part, value_part, tap_part, log_total, row_delta)

def reference(query, key, value, out_grad, query_gain, key_gain, rel_bias):
    block = PREV * SEG
    score_scale = HD ** (-0.5)
    shape = (TOKENS, H, HD)
    query_unit, query_scale, query_hat = normalize(query.reshape(shape), query_gain)
    key_unit, key_scale, key_hat = normalize(key.reshape(shape), key_gain)
    padding = jnp.zeros((block, H, HD), jnp.bfloat16)
    key_heads = jnp.concatenate([padding, key_hat]).transpose(1, 0, 2)
    value_heads = jnp.concatenate([padding, value.reshape(shape)]).transpose(1, 0, 2)
    query_heads = query_hat.transpose(1, 0, 2)
    grad_heads = out_grad.reshape(shape).transpose(1, 0, 2)
    inside = band_mask(block)
    later = jnp.arange(2 * block, dtype=jnp.int32)[None, :] >= block
    block_count = TOKENS // block

    def per_head(items):
        query_rows, key_rows, value_rows, grad_rows, table_row = items
        bias_block = bias_matrix(table_row, block)

        def per_block(block_index):
            row_start = (block_index * block).astype(jnp.int32)
            allowed = inside & (later | (block_index > 0))
            query_block = lax.dynamic_slice_in_dim(query_rows, row_start, block, 0)
            key_block = lax.dynamic_slice_in_dim(key_rows, row_start, 2 * block, 0)
            value_block = lax.dynamic_slice_in_dim(value_rows, row_start, 2 * block, 0)
            grad_block = lax.dynamic_slice_in_dim(grad_rows, row_start, block, 0)
            results = block_gradients(query_block, key_block, value_block, grad_block, bias_block, allowed, score_scale, 0)
            return (results[0], results[1], results[2], results[3])
        query_part, key_part, value_part, tap_part = lax.map(per_block, jnp.arange(block_count, dtype=jnp.int32))
        key_sum = jnp.pad(key_part[:, :block].reshape(-1, HD), ((0, block), (0, 0))) + jnp.pad(key_part[:, block:].reshape(-1, HD), ((block, 0), (0, 0)))
        value_sum = jnp.pad(value_part[:, :block].reshape(-1, HD), ((0, block), (0, 0))) + jnp.pad(value_part[:, block:].reshape(-1, HD), ((block, 0), (0, 0)))
        return (query_part.reshape(-1, HD), key_sum[block:], value_sum[block:], lax.optimization_barrier(jnp.sum(tap_part, axis=0)))
    query_hat_grad, key_hat_grad, value_sum, bias_grad = lax.map(per_head, (query_heads, key_heads, value_heads, grad_heads, rel_bias))
    query_grad, query_gain_grad = norm_backward(query_hat_grad.transpose(1, 0, 2), query_unit, query_scale, query_gain)
    key_grad, key_gain_grad = norm_backward(key_hat_grad.transpose(1, 0, 2), key_unit, key_scale, key_gain)
    value_grad = value_sum.transpose(1, 0, 2).reshape(TOKENS, ATT)
    return (query_grad.reshape(TOKENS, ATT).astype(jnp.bfloat16), key_grad.reshape(TOKENS, ATT).astype(jnp.bfloat16), value_grad.astype(jnp.bfloat16), query_gain_grad, key_gain_grad, bias_grad)
```

```python
import functools

import jax
import jax.numpy as jnp
from jax import lax
from jax.experimental import pallas as pl
from jax.experimental.pallas import tpu as pltpu
from jax.sharding import PartitionSpec as P

SEG = 64
PREV = 8
CLIP = 128
LANES = 128
TILE = 128

epsilon = 1e-06
f32 = jnp.float32
bf16 = jnp.bfloat16

ROWS_COLS = (((1,), (1,)), ((), ()))
ROWS_ROWS = (((0,), (0,)), ((), ()))


def shifted(block, axis, distance):
    devices = range(lax.axis_size(axis))
    route = [(i - distance, i) for i in devices if i - distance in devices]
    return lax.ppermute(block, axis, route)


def iota(shape, dim):
    return lax.broadcasted_iota(jnp.int32, shape, dim)


def head_mean(x, head_width):
    same = iota((LANES, LANES), 0) // head_width == iota((LANES, LANES), 1) // head_width
    ones = jnp.where(same, 1.0 / head_width, 0.0).astype(bf16)
    high = x.astype(bf16)
    low = (x - high.astype(f32)).astype(bf16)
    return jnp.dot(high, ones, preferred_element_type=f32) + jnp.dot(
        low, ones, preferred_element_type=f32
    )


def exact_dot(selector, x):
    high = x.astype(bf16)
    low = (x - high.astype(f32)).astype(bf16)
    return jnp.dot(selector, high, preferred_element_type=f32) + jnp.dot(
        selector, low, preferred_element_type=f32
    )


def unit_and_scale(rows, head_width):
    widened = rows.astype(f32)
    scale = lax.rsqrt(head_mean(widened * widened, head_width) + epsilon)
    return widened * scale, scale


def norm_backward(grad_hat, unit, scale, gain, head_width):
    grad_unit = grad_hat * gain
    inner = head_mean(grad_unit * unit, head_width)
    return scale * (grad_unit - unit * inner)


def rows8(x):
    return jnp.sum(x.reshape(x.shape[0] // 8, 8, x.shape[1]), axis=0)


def main_kernel(
    head_width,
    has_before,
    q_ref,
    k_ref,
    v_ref,
    g_ref,
    kr_ref,
    vr_ref,
    q_gain_ref,
    k_gain_ref,
    near_ref,
    dq_ref,
    dk_ref,
    dv_ref,
    dkr_ref,
    dvr_ref,
    stats_ref,
    qs,
    gs,
    kh,
    ku,
    ebuf,
    dbuf,
    pbuf,
    sbuf,
):
    pair = pl.program_id(0)
    rows = q_ref.shape[0]
    tiles = rows // TILE
    wide = 2 * TILE
    score_scale = head_width ** (-0.5)
    before = has_before[0].astype(f32)
    q_gain = q_gain_ref[...]
    k_gain = k_gain_ref[...]

    for part, ref in enumerate((kr_ref, k_ref)):
        unit, _ = unit_and_scale(ref[...], head_width)
        ku[pl.ds(part * rows, rows), :] = unit
        kh[pl.ds(part * rows, rows), :] = (unit * k_gain).astype(bf16)

    lane = iota((TILE, LANES), 1)
    first = lane < head_width
    q_unit, q_scale = unit_and_scale(q_ref[...], head_width)
    q_hat = (q_unit * q_gain).astype(bf16)
    zero = jnp.zeros((TILE, LANES), bf16)
    for b in range(tiles):
        part = q_hat[b * TILE : (b + 1) * TILE, :] * jnp.asarray(score_scale, bf16)
        grad = g_ref[pl.ds(b * TILE, TILE), :]
        qs[pl.ds(b * wide, TILE), :] = jnp.where(first, part, zero)
        qs[pl.ds(b * wide + TILE, TILE), :] = jnp.where(first, zero, part)
        gs[pl.ds(b * wide, TILE), :] = jnp.where(first, grad, zero)
        gs[pl.ds(b * wide + TILE, TILE), :] = jnp.where(first, zero, grad)

    key_pos = iota((TILE, wide), 0)
    query_pos = iota((TILE, wide), 1) % TILE
    causal = query_pos >= key_pos
    inside = key_pos // SEG >= query_pos // SEG
    near = near_ref[pl.ds(2 * pair, 2), :]
    skewed = [
        pltpu.roll(
            jnp.broadcast_to(near[h : h + 1, :], (TILE, TILE)), 0, 1, stride=1, stride_axis=0
        )
        for h in range(2)
    ]
    bias = jnp.concatenate(skewed, axis=1)
    bias_below = jnp.where(causal, 0.0, bias)

    near_grad = jnp.zeros((TILE, wide), f32)
    total = jnp.zeros((1, wide), f32)
    q_gain_grad = jnp.zeros((1, LANES), f32)
    for b in range(tiles):
        q_tile = qs[pl.ds(b * wide, wide), :]
        g_tile = gs[pl.ds(b * wide, wide), :]
        own_sum = jnp.zeros((8, wide), f32)
        before_sum = jnp.zeros((8, wide), f32)
        weighted = jnp.zeros((8, wide), f32)
        for j in range(tiles + 1):
            a = b + j
            scores = lax.dot_general(
                kh[pl.ds(a * TILE, TILE), :], q_tile, ROWS_COLS, preferred_element_type=f32
            )
            if j == tiles:
                scores = scores + bias
            if j == tiles - 1:
                scores = scores + bias_below
            e = jnp.exp(scores)
            if j == tiles:
                e = jnp.where(causal, e, 0.0)
            if j == 0:
                e = jnp.where(inside, e, 0.0)
            v_tile = (
                vr_ref[pl.ds(a * TILE, TILE), :]
                if a < tiles
                else v_ref[pl.ds((a - tiles) * TILE, TILE), :]
            )
            d = lax.dot_general(v_tile, g_tile, ROWS_COLS, preferred_element_type=f32)
            if a < tiles:
                before_sum = before_sum + rows8(e)
            else:
                own_sum = own_sum + rows8(e)
            weighted = weighted + rows8(e * d)
            ebuf[pl.ds(j * TILE, TILE), :] = e
            dbuf[pl.ds(j * TILE, TILE), :] = d
        normalizer = jnp.sum(own_sum + before_sum * before, axis=0, keepdims=True)
        weighted = jnp.sum(weighted, axis=0, keepdims=True)
        inverse = 1.0 / normalizer
        delta = weighted * inverse
        inverse_before = inverse * before
        total = total + (weighted - delta * normalizer) * inverse
        for j in range(tiles + 1):
            a = b + j
            attention = ebuf[pl.ds(j * TILE, TILE), :] * (
                inverse_before if a < tiles else inverse
            )
            score_grad = attention * (dbuf[pl.ds(j * TILE, TILE), :] - delta)
            if j == tiles:
                near_grad = near_grad + score_grad
            if j == tiles - 1:
                near_grad = near_grad + jnp.where(causal, 0.0, score_grad)
            pbuf[pl.ds(a * TILE, TILE), pl.ds(b * wide, wide)] = attention.astype(bf16)
            sbuf[pl.ds(a * TILE, TILE), pl.ds(b * wide, wide)] = score_grad.astype(bf16)
        span = (tiles + 1) * TILE
        turned = lax.dot_general(
            kh[pl.ds(b * TILE, span), :],
            sbuf[pl.ds(b * TILE, span), pl.ds(b * wide, wide)],
            ROWS_ROWS,
            preferred_element_type=f32,
        )
        turned = jnp.concatenate([turned[:head_width, :TILE], turned[head_width:, TILE:]], axis=0)
        grad_hat = turned.T * score_scale
        rows_b = slice(b * TILE, (b + 1) * TILE)
        unit = q_unit[rows_b, :]
        dq_ref[pl.ds(b * TILE, TILE), :] = norm_backward(
            grad_hat, unit, q_scale[rows_b, :], q_gain, head_width
        ).astype(bf16)
        q_gain_grad = q_gain_grad + jnp.sum(grad_hat * unit, axis=0, keepdims=True)

    k_gain_grad = jnp.zeros((1, LANES), f32)
    for a in range(2 * tiles):
        low, high = max(0, a - tiles), min(tiles - 1, a)
        at = pl.ds(low * wide, (high - low + 1) * wide)
        keys = pl.ds(a * TILE, TILE)
        dv = jnp.dot(pbuf[keys, at], gs[at, :], preferred_element_type=f32)
        dk = jnp.dot(sbuf[keys, at], qs[at, :], preferred_element_type=f32)
        k_gain_grad = k_gain_grad + jnp.sum(dk * ku[keys, :], axis=0, keepdims=True)
        if a < tiles:
            dkr_ref[keys, :] = dk.astype(bf16)
            dvr_ref[keys, :] = dv.astype(bf16)
        else:
            own = pl.ds((a - tiles) * TILE, TILE)
            dk_ref[own, :] = dk
            dv_ref[own, :] = dv

    @pl.when(pair == 0)
    def _():
        stats_ref[...] = jnp.zeros_like(stats_ref)

    heads = near_ref.shape[0]
    one_lane = iota((1, LANES), 1)
    flip = iota((TILE, TILE), 0) + iota((TILE, TILE), 1) == TILE - 1
    near_grad = exact_dot(jnp.where(flip, 1.0, 0.0).astype(bf16), near_grad)
    last = jnp.zeros((1, LANES), f32)
    for h in range(2):
        half = slice(h * TILE, (h + 1) * TILE)
        straight = pltpu.roll(near_grad[:, half], 1, 1, stride=1, stride_axis=0)
        taps = jnp.sum(straight, axis=0, keepdims=True)
        stats_ref[pl.ds(2 * pair + h, 1), :] = taps
        rest = jnp.sum(total[:, half] - taps, axis=1, keepdims=True)
        last = last + jnp.where(one_lane == 2 * pair + h, rest, 0.0)
    q_fold = q_gain_grad + pltpu.roll(q_gain_grad, head_width, 1)
    k_fold = k_gain_grad + pltpu.roll(k_gain_grad, head_width, 1)
    stats_ref[pl.ds(heads, 1), :] += jnp.where(one_lane < head_width, q_fold, k_fold)
    stats_ref[pl.ds(heads + 1, 1), :] += last


def final_kernel(
    head_width,
    tp_index,
    k_ref,
    k_gain_ref,
    dk_ref,
    dv_ref,
    dkb_ref,
    dvb_ref,
    all_ref,
    dk_out,
    dv_out,
    q_gain_out,
    k_gain_out,
    bias_out,
):
    unit, scale = unit_and_scale(k_ref[...], head_width)
    grad_hat = dk_ref[...] + dkb_ref[...].astype(f32)
    dk_out[...] = norm_backward(grad_hat, unit, scale, k_gain_ref[...], head_width).astype(bf16)
    dv_out[...] = (dv_ref[...] + dvb_ref[...].astype(f32)).astype(bf16)
    heads = bias_out.shape[0]

    @pl.when(pl.program_id(0) == 0)
    def _():
        everyone = jnp.sum(all_ref[...], axis=0)
        gains = jnp.sum(everyone[:, heads : heads + 1, :], axis=0)
        q_gain_out[...] = gains[:, :head_width]
        k_gain_out[...] = gains[:, head_width:]
        mine = iota(everyone.shape, 0) == tp_index[0]
        summed = jnp.sum(jnp.where(mine, everyone, 0.0), axis=0)
        bias_out[:, :CLIP] = summed[:heads, :]
        row = iota((heads, LANES), 0)
        column = iota((heads, LANES), 1)
        last = jnp.sum(
            jnp.where(row == column, summed[heads + 1 : heads + 2, :], 0.0), axis=1, keepdims=True
        )
        bias_out[:, CLIP:] = last


def per_device(query, key, value, out_grad, query_gain, key_gain, rel_bias):
    rows, width = query.shape
    heads = rel_bias.shape[0]
    head_width = width // heads
    pairs = width // LANES
    copies = LANES // head_width
    before_key = shifted(key, "sp", 1)
    before_value = shifted(value, "sp", 1)
    q_gain = jnp.tile(query_gain[None, :], (1, copies))
    k_gain = jnp.tile(key_gain[None, :], (1, copies))
    near = rel_bias[:, :CLIP] - rel_bias[:, CLIP:]
    has_before = (lax.axis_index("sp") > 0).astype(jnp.int32).reshape(1)
    column = pl.BlockSpec((rows, LANES), lambda p: (0, p))
    whole = lambda shape: pl.BlockSpec(shape, lambda p: (0,) * len(shape))
    stat_rows = -(-(heads + 2) // 8) * 8
    sds = jax.ShapeDtypeStruct
    dq, dk, dv, dk_before, dv_before, stats = pl.pallas_call(
        functools.partial(main_kernel, head_width),
        grid=(pairs,),
        in_specs=[pl.BlockSpec(memory_space=pltpu.SMEM)]
        + [column] * 6
        + [whole((1, LANES)), whole((1, LANES)), whole((heads, CLIP))],
        out_specs=[column] * 5 + [whole((stat_rows, LANES))],
        out_shape=[
            sds((rows, width), bf16),
            sds((rows, width), f32),
            sds((rows, width), f32),
            sds((rows, width), bf16),
            sds((rows, width), bf16),
            sds((stat_rows, LANES), f32),
        ],
        scratch_shapes=[
            pltpu.VMEM((2 * rows, LANES), bf16),
            pltpu.VMEM((2 * rows, LANES), bf16),
            pltpu.VMEM((2 * rows, LANES), bf16),
            pltpu.VMEM((2 * rows, LANES), f32),
            pltpu.VMEM((rows + TILE, 2 * TILE), f32),
            pltpu.VMEM((rows + TILE, 2 * TILE), f32),
            pltpu.VMEM((2 * rows, 2 * rows), bf16),
            pltpu.VMEM((2 * rows, 2 * rows), bf16),
        ],
        name="main",
    )(has_before, query, key, value, out_grad, before_key, before_value, q_gain, k_gain, near)
    dk_back = shifted(dk_before, "sp", -1)
    dv_back = shifted(dv_before, "sp", -1)
    axes = ("sp", "tp")
    members = (lax.axis_size("sp"), lax.axis_size("tp"))
    spread = jnp.broadcast_to(stats[None], (members[0] * members[1],) + stats.shape)
    everyone = lax.all_to_all(spread, axes, 0, 0, tiled=True).reshape(members + stats.shape)
    tp_index = lax.axis_index("tp").astype(jnp.int32).reshape(1)
    dk, dv, q_gain_grad, k_gain_grad, bias_grad = pl.pallas_call(
        functools.partial(final_kernel, head_width),
        grid=(pairs,),
        in_specs=[pl.BlockSpec(memory_space=pltpu.SMEM), column, whole((1, LANES))]
        + [column] * 4
        + [whole(everyone.shape)],
        out_specs=[column, column]
        + [whole((1, head_width)), whole((1, head_width)), whole((heads, CLIP + 1))],
        out_shape=[
            sds((rows, width), bf16),
            sds((rows, width), bf16),
            sds((1, head_width), f32),
            sds((1, head_width), f32),
            sds((heads, CLIP + 1), f32),
        ],
        name="final",
    )(tp_index, key, k_gain, dk, dv, dk_back, dv_back, everyone)
    return (dq, dk, dv, q_gain_grad[0], k_gain_grad[0], bias_grad)


def solution(mesh):
    placed = (P("sp", "tp"), P("sp", "tp"), P("sp", "tp"), P("sp", "tp"), P(), P(), P("tp", None))
    return jax.shard_map(
        per_device,
        mesh=mesh,
        in_specs=placed,
        out_specs=(P("sp", "tp"), P("sp", "tp"), P("sp", "tp"), P(), P(), P("tp", None)),
        check_vma=False,
    )
```

```python
import jax
import jax.numpy as jnp
from jax import lax
from jax.experimental import pallas as pl
from jax.experimental.pallas import tpu as pltpu
from jax.sharding import PartitionSpec as P


SEG = 64
CLIP = 128
LANES = 128
TILE = 128
WIDE = 2 * TILE
GRANT = 12 * 1024 * 1024

epsilon = 1e-06
f32 = jnp.float32
bf16 = jnp.bfloat16

ROWS_COLS = (((1,), (1,)), ((), ()))


def shifted(block, axis, distance):
    devices = range(lax.axis_size(axis))
    route = [(i - distance, i) for i in devices if i - distance in devices]
    return lax.ppermute(block, axis, route)


def iota(shape, dim):
    return lax.broadcasted_iota(jnp.int32, shape, dim)


def split_dot(x, matrix):
    high = x.astype(bf16)
    low = (x - high.astype(f32)).astype(bf16)
    return jnp.dot(high, matrix, preferred_element_type=f32) + jnp.dot(
        low, matrix, preferred_element_type=f32
    )


def head_mean(x, head_width):
    same = iota((LANES, LANES), 0) // head_width == iota((LANES, LANES), 1) // head_width
    return split_dot(x, jnp.where(same, 1.0 / head_width, 0.0).astype(bf16))


def unit_and_scale(rows, head_width):
    widened = rows.astype(f32)
    scale = lax.rsqrt(head_mean(widened * widened, head_width) + epsilon)
    return widened * scale, scale


def norm_backward(grad_hat, unit, scale, gain, head_width):
    grad_unit = grad_hat * gain
    inner = head_mean(grad_unit * unit, head_width)
    return scale * (grad_unit - unit * inner)


def rows8(x):
    return jnp.sum(x.reshape(x.shape[0] // 8, 8, x.shape[1]), axis=0)


def both_heads(gain_ref):
    gain = gain_ref[...]
    return jnp.concatenate([gain] * (LANES // gain.shape[1]), axis=1)


def each_pair(pairs, body):
    for p in range(pairs):
        body(p)


def at(tile):
    return pl.ds(tile * TILE, TILE)


def masks():
    key_pos = iota((TILE, WIDE), 0)
    query_pos = iota((TILE, WIDE), 1) % TILE
    return query_pos >= key_pos, key_pos // SEG >= query_pos // SEG


def as_column(row, rows):
    turned = jnp.broadcast_to(row, (LANES, rows)).T
    return turned


def own_kernel(
    q_hbm, k_hbm, v_hbm, g_hbm, q_gain_hbm, k_gain_hbm, table_hbm,
    qs_ref, gs_ref, kt_ref, ku_ref, qu_ref, qscale_ref, e_ref, sum_ref, weighted_ref, bias_ref,
    gains_ref, kh_ref, q_ref, k_ref, v_ref, g_ref, q_gain_ref, k_gain_ref, table_ref, sems,
):
    sources = (q_gain_hbm, k_gain_hbm, table_hbm, k_hbm, q_hbm, g_hbm, v_hbm)
    targets = (q_gain_ref, k_gain_ref, table_ref, k_ref, q_ref, g_ref, v_ref)
    copies = [
        pltpu.make_async_copy(source, target, sems.at[i])
        for i, (source, target) in enumerate(zip(sources, targets))
    ]
    for copy in copies:
        copy.start()
    for copy in copies:
        copy.wait()
    rows = q_ref.shape[0]
    tiles = rows // TILE
    head_width = q_gain_ref.shape[1]
    q_gain, k_gain = both_heads(q_gain_ref), both_heads(k_gain_ref)
    gains_ref[...] = jnp.concatenate([q_gain, k_gain, jnp.zeros((6, LANES), f32)], axis=0)
    causal, _ = masks()
    first = iota((TILE, LANES), 1) < head_width
    zero = jnp.zeros((TILE, LANES), bf16)
    table = table_ref[...]
    near = table[:, :CLIP] - table[:, CLIP:]

    def body(p):
        lanes = pl.ds(p * LANES, LANES)
        unit, _ = unit_and_scale(k_ref[:, lanes], head_width)
        ku_ref[p] = unit
        hat = (unit * k_gain).astype(bf16)
        kh_ref[p] = hat
        kt_ref[p] = hat.T
        unit, scale = unit_and_scale(q_ref[:, lanes], head_width)
        qu_ref[p] = unit
        qscale_ref[p] = scale
        hat = (unit * q_gain).astype(bf16) * jnp.asarray(head_width ** (-0.5), bf16)
        for b in range(tiles):
            part = hat[b * TILE : (b + 1) * TILE, :]
            grad = g_ref[at(b), lanes]
            qs_ref[p, pl.ds(b * WIDE, TILE), :] = jnp.where(first, part, zero)
            qs_ref[p, pl.ds(b * WIDE + TILE, TILE), :] = jnp.where(first, zero, part)
            gs_ref[p, pl.ds(b * WIDE, TILE), :] = jnp.where(first, grad, zero)
            gs_ref[p, pl.ds(b * WIDE + TILE, TILE), :] = jnp.where(first, zero, grad)
        skewed = [
            pltpu.roll(
                jnp.broadcast_to(near[2 * p + h : 2 * p + h + 1, :], (TILE, TILE)),
                0,
                1,
                stride=1,
                stride_axis=0,
            )
            for h in range(2)
        ]
        bias = jnp.concatenate(skewed, axis=1)
        below = jnp.where(causal, 0.0, bias)
        bias_ref[p] = below
        for b in range(tiles):
            queries = pl.ds(b * WIDE, WIDE)
            q_tile, g_tile = qs_ref[p, queries, :], gs_ref[p, queries, :]
            total = jnp.zeros((8, WIDE), f32)
            weighted = jnp.zeros((8, WIDE), f32)
            for a in range(b + 1):
                scores = lax.dot_general(
                    kh_ref[p, at(a), :], q_tile, ROWS_COLS, preferred_element_type=f32
                )
                if a == b:
                    scores = scores + bias
                if a == b - 1:
                    scores = scores + below
                e = jnp.exp(scores)
                if a == b:
                    e = jnp.where(causal, e, 0.0)
                d = lax.dot_general(
                    v_ref[at(a), lanes], g_tile, ROWS_COLS, preferred_element_type=f32
                )
                total = total + rows8(e)
                weighted = weighted + rows8(e * d)
                e_ref[p, at(a), queries] = e.astype(bf16)
            sum_ref[p, :, queries] = total
            weighted_ref[p, :, queries] = weighted

    each_pair(qs_ref.shape[0], body)


def before_kernel(
    has_before, kr_ref, gains_ref, qs_ref, gs_ref, e_ref, sum_ref, bias_ref,
    krt_ref, kru_ref, er_ref, norm_ref, qn_ref, dv_ref, dvr_ref, krh_ref, gn_ref,
):
    rows, width = kr_ref.shape
    tiles = rows // TILE
    head_width = width // (2 * qs_ref.shape[0])
    before = has_before[0].astype(f32)
    k_gain = gains_ref[1:2, :]
    _, inside = masks()

    def body(p):
        lanes = pl.ds(p * LANES, LANES)
        unit, _ = unit_and_scale(kr_ref[:, lanes], head_width)
        kru_ref[p] = unit
        hat = (unit * k_gain).astype(bf16)
        krh_ref[p] = hat
        krt_ref[p] = hat.T
        for b in range(tiles):
            queries = pl.ds(b * WIDE, WIDE)
            q_tile = qs_ref[p, queries, :]
            total = jnp.zeros((8, WIDE), f32)
            for a in range(b, tiles):
                scores = lax.dot_general(
                    krh_ref[p, at(a), :], q_tile, ROWS_COLS, preferred_element_type=f32
                )
                if b == 0 and a == tiles - 1:
                    scores = scores + bias_ref[p]
                e = jnp.exp(scores)
                if a == b:
                    e = jnp.where(inside, e, 0.0)
                total = total + rows8(e)
                er_ref[p, at(a), queries] = e.astype(bf16)
            normalizer = jnp.sum(
                sum_ref[p, :, queries] + total * before, axis=0, keepdims=True
            )
            norm_ref[p, :, queries] = jnp.broadcast_to(normalizer, (8, WIDE))
            column = as_column(1.0 / normalizer, WIDE)
            qn_ref[p, queries, :] = (q_tile.astype(f32) * column).astype(bf16)
            gn_ref[queries, :] = (gs_ref[p, queries, :].astype(f32) * column).astype(bf16)
        for a in range(tiles):
            span = pl.ds(0, (a + 1) * WIDE)
            dvr_ref[at(a), lanes] = jnp.dot(
                er_ref[p, at(a), span], gn_ref[span, :], preferred_element_type=f32
            ).astype(bf16)
        for a in range(tiles):
            span = pl.ds(a * WIDE, (tiles - a) * WIDE)
            dv_ref[at(a), lanes] = jnp.dot(
                e_ref[p, at(a), span], gn_ref[span, :], preferred_element_type=f32
            )

    each_pair(qs_ref.shape[0], body)


def grad_kernel(
    has_before, vr_ref, v_ref, gs_ref, qn_ref, kt_ref, krt_ref, ku_ref, kru_ref, qu_ref,
    qscale_ref, e_ref, er_ref, norm_ref, weighted_ref, gains_ref,
    dq_ref, dk_ref, dkr_ref, stats_ref, s_ref, sr_ref, delta_ref, turned_ref,
):
    rows, width = v_ref.shape
    tiles = rows // TILE
    pairs = qn_ref.shape[0]
    heads = 2 * pairs
    head_width = width // heads
    before = has_before[0].astype(f32)
    q_gain = gains_ref[0:1, :]
    causal, _ = masks()
    one_lane = iota((1, LANES), 1)
    flip = iota((TILE, TILE), 0) + iota((TILE, TILE), 1) == TILE - 1
    flip = jnp.where(flip, 1.0, 0.0).astype(bf16)

    for p in range(pairs):
        lanes = pl.ds(p * LANES, LANES)
        for b in range(tiles):
            queries = pl.ds(b * WIDE, WIDE)
            g_tile = gs_ref[p, queries, :]
            weighted = weighted_ref[p, :, queries]
            for a in range(b, tiles):
                d = lax.dot_general(
                    vr_ref[at(a), lanes], g_tile, ROWS_COLS, preferred_element_type=f32
                )
                weighted = weighted + rows8(er_ref[p, at(a), queries].astype(f32) * d)
            weighted = jnp.sum(weighted, axis=0, keepdims=True)
            normalizer = norm_ref[p, 0:1, queries]
            inverse = 1.0 / normalizer
            delta = weighted * inverse
            rest = (weighted - delta * normalizer) * inverse
            delta_ref[p, :, queries] = jnp.concatenate([inverse, delta, rest], axis=0)
    for p in range(pairs):
        lanes = pl.ds(p * LANES, LANES)
        for b in range(tiles):
            queries = pl.ds(b * WIDE, WIDE)
            g_tile = gs_ref[p, queries, :]
            delta = delta_ref[p, 1:2, queries]
            for a in range(b, tiles):
                d = lax.dot_general(
                    vr_ref[at(a), lanes], g_tile, ROWS_COLS, preferred_element_type=f32
                )
                s = er_ref[p, at(a), queries].astype(f32) * (d - delta)
                sr_ref[p, at(a), queries] = s.astype(bf16)
            for a in range(b + 1):
                d = lax.dot_general(
                    v_ref[at(a), lanes], g_tile, ROWS_COLS, preferred_element_type=f32
                )
                s = e_ref[p, at(a), queries].astype(f32) * (d - delta)
                s_ref[p, at(a), queries] = s.astype(bf16)
    for p in range(pairs):
        for b in range(tiles):
            queries = pl.ds(b * WIDE, WIDE)
            own, old = pl.ds(0, (b + 1) * TILE), pl.ds(b * TILE, (tiles - b) * TILE)
            turned = jnp.dot(
                kt_ref[p, :, own], s_ref[p, own, queries], preferred_element_type=f32
            ) + jnp.dot(
                krt_ref[p, :, old], sr_ref[p, old, queries], preferred_element_type=f32
            )
            turned = turned * (delta_ref[p, 0:1, queries] * head_width ** (-0.5))
            turned = jnp.concatenate(
                [turned[:head_width, :TILE], turned[head_width:, TILE:]], axis=0
            )
            turned_ref[p, at(b), :] = turned.T
    k_sum = jnp.zeros((1, LANES), f32)
    q_sum = jnp.zeros((1, LANES), f32)
    for p in range(pairs):
        lanes = pl.ds(p * LANES, LANES)
        for a in range(tiles):
            span = pl.ds(0, (a + 1) * WIDE)
            dk = jnp.dot(sr_ref[p, at(a), span], qn_ref[p, span, :], preferred_element_type=f32)
            k_sum = k_sum + jnp.sum(dk * kru_ref[p, at(a), :], axis=0, keepdims=True)
            dkr_ref[at(a), lanes] = dk.astype(bf16)
        for a in range(tiles):
            span = pl.ds(a * WIDE, (tiles - a) * WIDE)
            dk = jnp.dot(s_ref[p, at(a), span], qn_ref[p, span, :], preferred_element_type=f32)
            k_sum = k_sum + jnp.sum(dk * ku_ref[p, at(a), :], axis=0, keepdims=True)
            dk_ref[at(a), lanes] = dk
    lines = []
    last = jnp.zeros((1, LANES), f32)
    for p in range(pairs):
        lanes = pl.ds(p * LANES, LANES)
        grad_hat = turned_ref[p]
        unit = qu_ref[p]
        dq_ref[:, lanes] = norm_backward(
            grad_hat, unit, qscale_ref[p], q_gain, head_width
        ).astype(bf16)
        q_sum = q_sum + jnp.sum(grad_hat * unit, axis=0, keepdims=True)
        near_grad = jnp.zeros((TILE, WIDE), f32)
        total = jnp.zeros((1, WIDE), f32)
        for b in range(tiles):
            queries = pl.ds(b * WIDE, WIDE)
            inverse = delta_ref[p, 0:1, queries]
            total = total + delta_ref[p, 2:3, queries]
            below = s_ref[p, at(b - 1), queries] if b else sr_ref[p, at(tiles - 1), queries]
            below = below.astype(f32) * (inverse if b else inverse * before)
            exact = s_ref[p, at(b), queries].astype(f32) * inverse
            near_grad = near_grad + jnp.where(causal, exact, below)
        near_grad = split_dot_left(flip, near_grad)
        for h in range(2):
            half = slice(h * TILE, (h + 1) * TILE)
            straight = pltpu.roll(near_grad[:, half], 1, 1, stride=1, stride_axis=0)
            taps = jnp.sum(straight, axis=0, keepdims=True)
            lines.append(taps)
            rest = jnp.sum(total[:, half] - taps, axis=1, keepdims=True)
            last = last + jnp.where(one_lane == 2 * p + h, rest, 0.0)
    q_fold = q_sum + pltpu.roll(q_sum, head_width, 1)
    k_fold = k_sum + pltpu.roll(k_sum, head_width, 1)
    lines.append(jnp.where(one_lane < head_width, q_fold, k_fold))
    lines.append(last)
    lines.append(jnp.zeros((stats_ref.shape[1] - len(lines), LANES), f32))
    stats_ref[...] = jnp.broadcast_to(jnp.concatenate(lines, axis=0)[None], stats_ref.shape)


def split_dot_left(matrix, x):
    high = x.astype(bf16)
    low = (x - high.astype(f32)).astype(bf16)
    return jnp.dot(matrix, high, preferred_element_type=f32) + jnp.dot(
        matrix, low, preferred_element_type=f32
    )


def final_kernel(
    tp_index, gains_ref, k_ref, dk_ref, dv_ref, dkb_ref, dvb_ref, all_ref,
    dk_out, dv_out, q_gain_out, k_gain_out, bias_out,
):
    _, width = dk_ref.shape
    head_width = width // bias_out.shape[0]
    k_gain = gains_ref[1:2, :]

    def body(p):
        lanes = pl.ds(p * LANES, LANES)
        unit, scale = unit_and_scale(k_ref[:, lanes], head_width)
        grad_hat = dk_ref[:, lanes] + dkb_ref[:, lanes].astype(f32)
        dk_out[:, lanes] = norm_backward(grad_hat, unit, scale, k_gain, head_width).astype(bf16)
        dv_out[:, lanes] = (dv_ref[:, lanes] + dvb_ref[:, lanes].astype(f32)).astype(bf16)

    each_pair(width // LANES, body)
    heads = bias_out.shape[0]
    everyone = jnp.sum(all_ref[...], axis=0)
    gains = jnp.sum(everyone[:, heads : heads + 1, :], axis=0)
    q_gain_out[...] = gains[:, :head_width]
    k_gain_out[...] = gains[:, head_width:]
    mine = iota(everyone.shape, 0) == tp_index[0]
    summed = jnp.sum(jnp.where(mine, everyone, 0.0), axis=0)
    bias_out[:, :CLIP] = summed[:heads, :]
    diagonal = iota((heads, LANES), 0) == iota((heads, LANES), 1)
    last = jnp.where(diagonal, summed[heads + 1 : heads + 2, :], 0.0)
    bias_out[:, CLIP:] = jnp.sum(last, axis=1, keepdims=True)


def call(kernel, args, outs, scratch=(), scalars=0, hbm=0, flops=0):
    args = [
        pltpu.with_memory_space_constraint(x, pltpu.HBM) if scalars <= i < scalars + hbm else x
        for i, x in enumerate(args)
    ]
    specs = [pl.BlockSpec(memory_space=pltpu.SMEM)] * scalars
    specs += [pl.BlockSpec(memory_space=pltpu.HBM)] * hbm
    specs += [pl.BlockSpec(memory_space=pltpu.VMEM)] * (len(args) - scalars - hbm)
    return pl.pallas_call(
        kernel,
        in_specs=specs,
        out_specs=[pl.BlockSpec(memory_space=pltpu.VMEM)] * len(outs),
        out_shape=[jax.ShapeDtypeStruct(*o) for o in outs],
        scratch_shapes=list(scratch),
        compiler_params=pltpu.CompilerParams(vmem_limit_bytes=GRANT),
        cost_estimate=pl.CostEstimate(flops=flops, bytes_accessed=0, transcendentals=0),
    )(*args)


def per_device(query, key, value, out_grad, query_gain, key_gain, rel_bias):
    rows, width = query.shape
    heads = rel_bias.shape[0]
    head_width = width // heads
    pairs = width // LANES
    double = 2 * rows
    before_key = shifted(key, "sp", 1)
    before_value = shifted(value, "sp", 1)
    q_gain, k_gain = query_gain[None, :], key_gain[None, :]
    has_before = (lax.axis_index("sp") > 0).astype(jnp.int32).reshape(1)
    tp_index = lax.axis_index("tp").astype(jnp.int32).reshape(1)
    stacked = ((pairs, double, LANES), bf16)
    hats = ((pairs, rows, LANES), bf16)
    turned = ((pairs, LANES, rows), bf16)
    units = ((pairs, rows, LANES), f32)
    square = ((pairs, rows, double), bf16)
    line = ((pairs, 8, double), f32)
    flat, flat_low = ((rows, width), f32), ((rows, width), bf16)
    gains = ((8, LANES), f32)
    qs, gs, kt, ku, qu, q_scale, e, sums, weighted, bias, gains = call(
        own_kernel,
        (query, key, value, out_grad, q_gain, k_gain, rel_bias),
        (stacked, stacked, turned, units, units, units, square, line, line,
         ((pairs, TILE, WIDE), f32), gains),
        scratch=[pltpu.VMEM(*hats)]
        + [pltpu.VMEM(*flat_low)] * 4
        + [pltpu.VMEM(q_gain.shape, f32), pltpu.VMEM(k_gain.shape, f32)]
        + [pltpu.VMEM(rel_bias.shape, f32), pltpu.SemaphoreType.DMA((7,))],
        hbm=7,
        flops=4_000_000_000,
    )
    krt, kru, er, norm, qn, dv, dv_before = call(
        before_kernel,
        (has_before, before_key, gains, qs, gs, e, sums, bias),
        (turned, units, square, line, stacked, flat, flat_low),
        scratch=[pltpu.VMEM(*hats), pltpu.VMEM((double, LANES), bf16)],
        scalars=1,
        flops=4_000_000_000,
    )
    dv_back = shifted(dv_before, "sp", -1)
    stat_rows = -(-(heads + 2) // 8) * 8
    members = (lax.axis_size("sp"), lax.axis_size("tp"))
    dq, dk, dk_before, stats = call(
        grad_kernel,
        (has_before, before_value, value, gs, qn, kt, krt, ku, kru, qu, q_scale, e, er, norm,
         weighted, gains),
        (flat_low, flat, flat_low, ((members[0] * members[1], stat_rows, LANES), f32)),
        scratch=[pltpu.VMEM(*square), pltpu.VMEM(*square)]
        + [pltpu.VMEM((pairs, 3, double), f32), pltpu.VMEM(*units)],
        scalars=1,
        flops=8_000_000_000,
    )
    dk_back = shifted(dk_before, "sp", -1)
    everyone = lax.all_to_all(stats, ("sp", "tp"), 0, 0, tiled=True)
    everyone = everyone.reshape(members + (stat_rows, LANES))
    dk, dv, q_gain_grad, k_gain_grad, bias_grad = call(
        final_kernel,
        (tp_index, gains, key, dk, dv, dk_back, dv_back, everyone),
        (flat_low, flat_low, ((1, head_width), f32), ((1, head_width), f32),
         ((heads, CLIP + 1), f32)),
        scalars=1,
        flops=1_000_000_000,
    )
    return (dq, dk, dv, q_gain_grad[0], k_gain_grad[0], bias_grad)


def solution(mesh):
    placed = (P("sp", "tp"), P("sp", "tp"), P("sp", "tp"), P("sp", "tp"), P(), P(), P("tp", None))
    return jax.shard_map(
        per_device,
        mesh=mesh,
        in_specs=placed,
        out_specs=(P("sp", "tp"), P("sp", "tp"), P("sp", "tp"), P(), P(), P("tp", None)),
        check_vma=False,
    )
```

```python
import jax
import jax.numpy as jnp
from jax import lax
from jax.experimental import pallas as pl
from jax.experimental.pallas import tpu as pltpu
from jax.sharding import PartitionSpec as P


SEG = 64
CLIP = 128
LANES = 128
TILE = 128
WIDE = 2 * TILE
GRANT = 16 * 1024 * 1024

epsilon = 1e-06
f32 = jnp.float32
bf16 = jnp.bfloat16

ROWS_COLS = (((1,), (1,)), ((), ()))


def shifted(block, axis, distance):
    devices = range(lax.axis_size(axis))
    route = [(i - distance, i) for i in devices if i - distance in devices]
    return lax.ppermute(block, axis, route)


def iota(shape, dim):
    return lax.broadcasted_iota(jnp.int32, shape, dim)


def split_dot(x, matrix):
    high = x.astype(bf16)
    low = (x - high.astype(f32)).astype(bf16)
    return jnp.dot(high, matrix, preferred_element_type=f32) + jnp.dot(
        low, matrix, preferred_element_type=f32
    )


def head_mean(x, head_width):
    same = iota((LANES, LANES), 0) // head_width == iota((LANES, LANES), 1) // head_width
    return split_dot(x, jnp.where(same, 1.0 / head_width, 0.0).astype(bf16))


def unit_and_scale(rows, head_width):
    widened = rows.astype(f32)
    scale = lax.rsqrt(head_mean(widened * widened, head_width) + epsilon)
    return widened * scale, scale


def norm_backward(grad_hat, unit, scale, gain, head_width):
    grad_unit = grad_hat * gain
    inner = head_mean(grad_unit * unit, head_width)
    return scale * (grad_unit - unit * inner)


def rows8(x):
    return jnp.sum(x.reshape(x.shape[0] // 8, 8, x.shape[1]), axis=0)


def both_heads(gain_ref):
    gain = gain_ref[...]
    return jnp.concatenate([gain] * (LANES // gain.shape[1]), axis=1)


def each_pair(pairs, body):
    for p in range(pairs):
        body(p)


def at(tile):
    return pl.ds(tile * TILE, TILE)


def masks():
    key_pos = iota((TILE, WIDE), 0)
    query_pos = iota((TILE, WIDE), 1) % TILE
    return query_pos >= key_pos, key_pos // SEG >= query_pos // SEG


def as_column(row, rows):
    turned = jnp.broadcast_to(row, (LANES, rows)).T
    return turned


def own_kernel(
    q_hbm, k_hbm, v_hbm, g_hbm, q_gain_hbm, k_gain_hbm, table_hbm,
    qs_ref, gs_ref, kt_ref, qu_ref, e_ref, e32_ref, d32_ref, sum_ref, weighted_ref,
    bias_ref, gains_ref, kh_ref, q_ref, k_ref, v_ref, g_ref, q_gain_ref, k_gain_ref, table_ref, sems,
):
    sources = (q_gain_hbm, k_gain_hbm, table_hbm, k_hbm, q_hbm, g_hbm, v_hbm)
    targets = (q_gain_ref, k_gain_ref, table_ref, k_ref, q_ref, g_ref, v_ref)
    copies = [
        pltpu.make_async_copy(source, target, sems.at[i])
        for i, (source, target) in enumerate(zip(sources, targets))
    ]
    for copy in copies:
        copy.start()
    for copy in copies:
        copy.wait()
    rows = q_ref.shape[0]
    tiles = rows // TILE
    head_width = q_gain_ref.shape[1]
    q_gain, k_gain = both_heads(q_gain_ref), both_heads(k_gain_ref)
    gains_ref[...] = jnp.concatenate([q_gain, k_gain, jnp.zeros((6, LANES), f32)], axis=0)
    causal, _ = masks()
    first = iota((TILE, LANES), 1) < head_width
    zero = jnp.zeros((TILE, LANES), bf16)
    table = table_ref[...]
    near = table[:, :CLIP] - table[:, CLIP:]

    def body(p):
        lanes = pl.ds(p * LANES, LANES)
        unit, _ = unit_and_scale(k_ref[:, lanes], head_width)
        hat = (unit * k_gain).astype(bf16)
        kh_ref[p] = hat
        kt_ref[p] = hat.T
        unit, _ = unit_and_scale(q_ref[:, lanes], head_width)
        qu_ref[p] = unit
        hat = (unit * q_gain).astype(bf16) * jnp.asarray(head_width ** (-0.5), bf16)
        for b in range(tiles):
            part = hat[b * TILE : (b + 1) * TILE, :]
            grad = g_ref[at(b), lanes]
            qs_ref[p, pl.ds(b * WIDE, TILE), :] = jnp.where(first, part, zero)
            qs_ref[p, pl.ds(b * WIDE + TILE, TILE), :] = jnp.where(first, zero, part)
            gs_ref[p, pl.ds(b * WIDE, TILE), :] = jnp.where(first, grad, zero)
            gs_ref[p, pl.ds(b * WIDE + TILE, TILE), :] = jnp.where(first, zero, grad)
        skewed = [
            pltpu.roll(
                jnp.broadcast_to(near[2 * p + h : 2 * p + h + 1, :], (TILE, TILE)),
                0,
                1,
                stride=1,
                stride_axis=0,
            )
            for h in range(2)
        ]
        bias = jnp.concatenate(skewed, axis=1)
        below = jnp.where(causal, 0.0, bias)
        bias_ref[p] = below
        for b in range(tiles):
            queries = pl.ds(b * WIDE, WIDE)
            q_tile, g_tile = qs_ref[p, queries, :], gs_ref[p, queries, :]
            total = jnp.zeros((8, WIDE), f32)
            weighted = jnp.zeros((8, WIDE), f32)
            for a in range(b + 1):
                scores = lax.dot_general(
                    kh_ref[p, at(a), :], q_tile, ROWS_COLS, preferred_element_type=f32
                )
                if a == b:
                    scores = scores + bias
                if a == b - 1:
                    scores = scores + below
                e = jnp.exp(scores)
                if a == b:
                    e = jnp.where(causal, e, 0.0)
                d = lax.dot_general(
                    v_ref[at(a), lanes], g_tile, ROWS_COLS, preferred_element_type=f32
                )
                total = total + rows8(e)
                weighted = weighted + rows8(e * d)
                e_ref[p, at(a), queries] = e.astype(bf16)
                e32_ref[p, at(a), queries] = e
                d32_ref[p, at(a), queries] = d
            sum_ref[p, :, queries] = total
            weighted_ref[p, :, queries] = weighted

    each_pair(qs_ref.shape[0], body)


def before_kernel(
    has_before, kr_ref, gains_ref, qs_ref, gs_ref, kt_ref, e_ref, sum_ref, bias_ref,
    kts_ref, er32_ref, norm_ref, qn_ref, dv_ref, dvr_ref, krh_ref, gn_ref, er_ref,
):
    rows, width = kr_ref.shape
    tiles = rows // TILE
    head_width = width // (2 * qs_ref.shape[0])
    before = has_before[0].astype(f32)
    k_gain = gains_ref[1:2, :]
    _, inside = masks()

    def body(p):
        lanes = pl.ds(p * LANES, LANES)
        unit, _ = unit_and_scale(kr_ref[:, lanes], head_width)
        hat = (unit * k_gain).astype(bf16)
        krh_ref[p] = hat
        kts_ref[p, :, :rows] = hat.T
        kts_ref[p, :, rows:] = kt_ref[p]
        for b in range(tiles):
            queries = pl.ds(b * WIDE, WIDE)
            q_tile = qs_ref[p, queries, :]
            total = jnp.zeros((8, WIDE), f32)
            for a in range(b, tiles):
                scores = lax.dot_general(
                    krh_ref[p, at(a), :], q_tile, ROWS_COLS, preferred_element_type=f32
                )
                if b == 0 and a == tiles - 1:
                    scores = scores + bias_ref[p]
                e = jnp.exp(scores)
                if a == b:
                    e = jnp.where(inside, e, 0.0)
                total = total + rows8(e)
                er_ref[p, at(a), queries] = e.astype(bf16)
                er32_ref[p, at(a), queries] = e
            normalizer = jnp.sum(
                sum_ref[p, :, queries] + total * before, axis=0, keepdims=True
            )
            norm_ref[p, :, queries] = jnp.broadcast_to(normalizer, (8, WIDE))
            column = as_column(1.0 / normalizer, WIDE)
            qn_ref[p, queries, :] = (q_tile.astype(f32) * column).astype(bf16)
            gn_ref[queries, :] = (gs_ref[p, queries, :].astype(f32) * column).astype(bf16)
        for a in range(tiles):
            span = pl.ds(0, (a + 1) * WIDE)
            dvr_ref[at(a), lanes] = jnp.dot(
                er_ref[p, at(a), span], gn_ref[span, :], preferred_element_type=f32
            ).astype(bf16)
        for a in range(tiles):
            span = pl.ds(a * WIDE, (tiles - a) * WIDE)
            dv_ref[at(a), lanes] = jnp.dot(
                e_ref[p, at(a), span], gn_ref[span, :], preferred_element_type=f32
            )

    each_pair(qs_ref.shape[0], body)


def grad_kernel(
    has_before, vr_ref, dd_ref, gs_ref, qn_ref, kts_ref, qu_ref, e_ref, er_ref, norm_ref,
    weighted_ref,
    dq_ref, dk_ref, dkr_ref, stats_hbm, s_ref, d_ref, delta_ref, table_ref, sem,
):
    rows, width = vr_ref.shape
    tiles = rows // TILE
    pairs = qn_ref.shape[0]
    heads = 2 * pairs
    head_width = width // heads
    before = has_before[0].astype(f32)
    causal, _ = masks()
    one_lane = iota((1, LANES), 1)
    always = has_before[0] > -1
    still = has_before[0] > -2

    @pl.when(always)
    def _():
        for p in range(pairs):
            lanes = pl.ds(p * LANES, LANES)
            for b in range(tiles):
                queries = pl.ds(b * WIDE, WIDE)
                g_tile = gs_ref[p, queries, :]
                weighted = weighted_ref[p, :, queries]
                for a in range(b, tiles):
                    d = lax.dot_general(
                        vr_ref[at(a), lanes], g_tile, ROWS_COLS, preferred_element_type=f32
                    )
                    d_ref[p, at(a), queries] = d
                    weighted = weighted + rows8(er_ref[p, at(a), queries] * d)
                weighted = jnp.sum(weighted, axis=0, keepdims=True)
                normalizer = norm_ref[p, 0:1, queries]
                inverse = 1.0 / normalizer
                delta = weighted * inverse
                rest = (weighted - delta * normalizer) * inverse
                delta_ref[p, :, queries] = jnp.concatenate([inverse, delta, rest], axis=0)

    @pl.when(still)
    def _():
        for p in range(pairs):
            lanes = pl.ds(p * LANES, LANES)
            for b in range(tiles):
                queries = pl.ds(b * WIDE, WIDE)
                delta = delta_ref[p, 1:2, queries]
                for a in range(b, tiles):
                    s = er_ref[p, at(a), queries] * (d_ref[p, at(a), queries] - delta)
                    s_ref[p, at(a), queries] = s.astype(bf16)
                for a in range(b + 1):
                    s = e_ref[p, at(a), queries] * (dd_ref[p, at(a), queries] - delta)
                    s_ref[p, at(tiles + a), queries] = s.astype(bf16)

    @pl.when(still)
    def _():
        for p in range(pairs):
            for b in range(tiles):
                queries = pl.ds(b * WIDE, WIDE)
                span = pl.ds(b * TILE, rows + TILE)
                turned = jnp.dot(
                    kts_ref[p, :, span], s_ref[p, span, queries], preferred_element_type=f32
                )
                turned = jnp.concatenate(
                    [turned[:head_width, :TILE], turned[head_width:, TILE:]], axis=0
                )
                inverse = delta_ref[p, 0:1, queries] * head_width ** (-0.5)
                inverse = jnp.concatenate(
                    [
                        jnp.broadcast_to(inverse[:, :TILE], (head_width, TILE)),
                        jnp.broadcast_to(inverse[:, TILE:], (head_width, TILE)),
                    ],
                    axis=0,
                )
                dq_ref[p, at(b), :] = (turned * inverse).T

    @pl.when(still)
    def _():
        q_sum = jnp.zeros((8, LANES), f32)
        for p in range(pairs):
            q_sum = q_sum + rows8(dq_ref[p] * qu_ref[p])
        q_sum = jnp.sum(q_sum, axis=0, keepdims=True)
        flip = iota((TILE, TILE), 0) + iota((TILE, TILE), 1) == TILE - 1
        flip = jnp.where(flip, 1.0, 0.0).astype(bf16)
        lines = []
        last = jnp.zeros((1, LANES), f32)
        for p in range(pairs):
            near_grad = jnp.zeros((TILE, WIDE), f32)
            total = jnp.zeros((1, WIDE), f32)
            for b in range(tiles):
                queries = pl.ds(b * WIDE, WIDE)
                total = total + delta_ref[p, 2:3, queries]
                below = s_ref[p, at(tiles + b - 1), queries].astype(f32)
                if b == 0:
                    below = below * before
                both = jnp.where(causal, s_ref[p, at(tiles + b), queries].astype(f32), below)
                near_grad = near_grad + both * delta_ref[p, 0:1, queries]
            near_grad = split_dot_left(flip, near_grad)
            for h in range(2):
                half = slice(h * TILE, (h + 1) * TILE)
                straight = pltpu.roll(near_grad[:, half], 1, 1, stride=1, stride_axis=0)
                taps = jnp.sum(straight, axis=0, keepdims=True)
                lines.append(taps)
                rest = jnp.sum(total[:, half] - taps, axis=1, keepdims=True)
                last = last + jnp.where(one_lane == 2 * p + h, rest, 0.0)
        lines += high_and_low(q_sum + pltpu.roll(q_sum, head_width, 1))
        lines += high_and_low(last)
        empty = table_ref.shape[1] - len(lines)
        if empty:
            lines.append(jnp.zeros((empty, LANES), f32))
        table = jnp.concatenate(lines, axis=0).astype(bf16)
        table_ref[...] = jnp.broadcast_to(table[None], table_ref.shape)

    copy = pltpu.make_async_copy(table_ref, stats_hbm, sem)
    copy.start()
    for p in range(pairs):
        lanes = pl.ds(p * LANES, LANES)
        for a in range(2 * tiles):
            low, high = max(0, a - tiles), min(tiles - 1, a)
            span = pl.ds(low * WIDE, (high - low + 1) * WIDE)
            dk = jnp.dot(s_ref[p, at(a), span], qn_ref[p, span, :], preferred_element_type=f32)
            if a < tiles:
                dkr_ref[at(a), lanes] = dk.astype(bf16)
            else:
                dk_ref[p, at(a - tiles), :] = dk
    copy.wait()


def high_and_low(x):
    high = x.astype(bf16).astype(f32)
    return [high, x - high]


def split_dot_left(matrix, x):
    high = x.astype(bf16)
    low = (x - high.astype(f32)).astype(bf16)
    return jnp.dot(matrix, high, preferred_element_type=f32) + jnp.dot(
        matrix, low, preferred_element_type=f32
    )


def finish_kernel(
    gains_ref, dqh_ref, q_ref, k_ref, dk_ref, dv_ref, dkb_ref, dvb_ref, dq_out, dk_out, dv_out
):
    pairs = dqh_ref.shape[0]
    head_width = k_ref.shape[1] // (2 * pairs)
    q_gain, k_gain = gains_ref[0:1, :], gains_ref[1:2, :]

    def body(p):
        lanes = pl.ds(p * LANES, LANES)
        unit, scale = unit_and_scale(q_ref[:, lanes], head_width)
        dq_out[:, lanes] = norm_backward(dqh_ref[p], unit, scale, q_gain, head_width).astype(bf16)
        unit, scale = unit_and_scale(k_ref[:, lanes], head_width)
        grad_hat = dk_ref[p] + dkb_ref[:, lanes].astype(f32)
        dk_out[:, lanes] = norm_backward(grad_hat, unit, scale, k_gain, head_width).astype(bf16)
        dv_out[:, lanes] = (dv_ref[:, lanes] + dvb_ref[:, lanes].astype(f32)).astype(bf16)

    each_pair(pairs, body)


def total_kernel(tp_index, gains_ref, all_ref, q_gain_out, k_gain_out, bias_out):
    heads = bias_out.shape[0]
    head_width = q_gain_out.shape[1]
    everyone = jnp.sum(all_ref[...].astype(f32), axis=0)
    gains = jnp.sum(everyone[:, heads : heads + 2, :], axis=0)
    gains = gains[0:1, :] + gains[1:2, :]
    q_gain_out[...] = gains[:, :head_width]
    ratio = gains_ref[0:1, :head_width] / gains_ref[1:2, :head_width]
    k_gain_out[...] = gains[:, :head_width] * ratio
    mine = iota(everyone.shape, 0) == tp_index[0]
    summed = jnp.sum(jnp.where(mine, everyone, 0.0), axis=0)
    bias_out[:, :CLIP] = summed[:heads, :]
    last = summed[heads + 2 : heads + 3, :] + summed[heads + 3 : heads + 4, :]
    diagonal = iota((heads, LANES), 0) == iota((heads, LANES), 1)
    bias_out[:, CLIP:] = jnp.sum(jnp.where(diagonal, last, 0.0), axis=1, keepdims=True)


def call(kernel, args, outs, scratch=(), scalars=0, hbm=0, out_hbm=(), flops=0):
    args = [
        pltpu.with_memory_space_constraint(x, pltpu.HBM) if scalars <= i < scalars + hbm else x
        for i, x in enumerate(args)
    ]
    specs = [pl.BlockSpec(memory_space=pltpu.SMEM)] * scalars
    specs += [pl.BlockSpec(memory_space=pltpu.HBM)] * hbm
    specs += [pl.BlockSpec(memory_space=pltpu.VMEM)] * (len(args) - scalars - hbm)
    return pl.pallas_call(
        kernel,
        in_specs=specs,
        out_specs=[
            pl.BlockSpec(memory_space=pltpu.HBM if i in out_hbm else pltpu.VMEM)
            for i in range(len(outs))
        ],
        out_shape=[jax.ShapeDtypeStruct(*o) for o in outs],
        scratch_shapes=list(scratch),
        compiler_params=pltpu.CompilerParams(vmem_limit_bytes=GRANT),
        cost_estimate=pl.CostEstimate(flops=flops, bytes_accessed=0, transcendentals=0),
    )(*args)


def per_device(query, key, value, out_grad, query_gain, key_gain, rel_bias):
    rows, width = query.shape
    heads = rel_bias.shape[0]
    head_width = width // heads
    pairs = width // LANES
    double = 2 * rows
    before_key = shifted(key, "sp", 1)
    before_value = shifted(value, "sp", 1)
    q_gain, k_gain = query_gain[None, :], key_gain[None, :]
    has_before = (lax.axis_index("sp") > 0).astype(jnp.int32).reshape(1)
    tp_index = lax.axis_index("tp").astype(jnp.int32).reshape(1)
    stacked = ((pairs, double, LANES), bf16)
    hats = ((pairs, rows, LANES), bf16)
    turned = ((pairs, LANES, rows), bf16)
    units = ((pairs, rows, LANES), f32)
    square = ((pairs, rows, double), bf16)
    square32 = ((pairs, rows, double), f32)
    line = ((pairs, 8, double), f32)
    flat, flat_low = ((rows, width), f32), ((rows, width), bf16)
    gains = ((8, LANES), f32)
    qs, gs, kt, qu, e, e32, d32, sums, weighted, bias, gains = call(
        own_kernel,
        (query, key, value, out_grad, q_gain, k_gain, rel_bias),
        (stacked, stacked, turned, units, square, square32, square32, line, line,
         ((pairs, TILE, WIDE), f32), gains),
        scratch=[pltpu.VMEM(*hats)]
        + [pltpu.VMEM(*flat_low)] * 4
        + [pltpu.VMEM(q_gain.shape, f32), pltpu.VMEM(k_gain.shape, f32)]
        + [pltpu.VMEM(rel_bias.shape, f32), pltpu.SemaphoreType.DMA((7,))],
        hbm=7,
        flops=4_000_000_000,
    )
    kts, er32, norm, qn, dv, dv_before = call(
        before_kernel,
        (has_before, before_key, gains, qs, gs, kt, e, sums, bias),
        (((pairs, LANES, double), bf16), square32, line, stacked, flat, flat_low),
        scratch=[pltpu.VMEM(*hats), pltpu.VMEM((double, LANES), bf16), pltpu.VMEM(*square)],
        scalars=1,
        flops=4_000_000_000,
    )
    dv_back = shifted(dv_before, "sp", -1)
    stat_rows = -(-(heads + 4) // 8) * 8
    members = (lax.axis_size("sp"), lax.axis_size("tp"))
    spread = ((members[0] * members[1], stat_rows, LANES), bf16)
    dq_hat, dk, dk_before, stats = call(
        grad_kernel,
        (has_before, before_value, d32, gs, qn, kts, qu, e32, er32, norm, weighted),
        (units, units, flat_low, spread),
        out_hbm=(3,),
        scratch=[pltpu.VMEM((pairs, double, double), bf16), pltpu.VMEM(*square32)]
        + [pltpu.VMEM((pairs, 3, double), f32), pltpu.VMEM(*spread), pltpu.SemaphoreType.DMA],
        scalars=1,
        flops=8_000_000_000,
    )
    dk_back = shifted(dk_before, "sp", -1)
    everyone = lax.all_to_all(stats, ("sp", "tp"), 0, 0, tiled=True)
    everyone = everyone.reshape(members + (stat_rows, LANES))
    dq, dk, dv = call(
        finish_kernel,
        (gains, dq_hat, query, key, dk, dv, dk_back, dv_back),
        (flat_low, flat_low, flat_low),
        flops=1_000_000_000,
    )
    q_gain_grad, k_gain_grad, bias_grad = call(
        total_kernel,
        (tp_index, gains, everyone),
        (((1, head_width), f32), ((1, head_width), f32), ((heads, CLIP + 1), f32)),
        scalars=1,
        flops=1_000_000,
    )
    return (dq, dk, dv, q_gain_grad[0], k_gain_grad[0], bias_grad)


def solution(mesh):
    placed = (P("sp", "tp"), P("sp", "tp"), P("sp", "tp"), P("sp", "tp"), P(), P(), P("tp", None))
    return jax.shard_map(
        per_device,
        mesh=mesh,
        in_specs=placed,
        out_specs=(P("sp", "tp"), P("sp", "tp"), P("sp", "tp"), P(), P(), P("tp", None)),
        check_vma=False,
    )
```

```python
import jax
import jax.numpy as jnp
from jax import lax
from jax.experimental import pallas as pl
from jax.experimental.pallas import tpu as pltpu
from jax.sharding import PartitionSpec as P


SEG = 64
CLIP = 128
LANES = 128
TILE = 128
WIDE = 2 * TILE
GRANT = 16 * 1024 * 1024

epsilon = 1e-06
f32 = jnp.float32
bf16 = jnp.bfloat16

ROWS_COLS = (((1,), (1,)), ((), ()))


def shifted(block, axis, distance):
    devices = range(lax.axis_size(axis))
    route = [(i - distance, i) for i in devices if i - distance in devices]
    return lax.ppermute(block, axis, route)


def iota(shape, dim):
    return lax.broadcasted_iota(jnp.int32, shape, dim)


def split_dot(x, matrix):
    high = x.astype(bf16)
    low = (x - high.astype(f32)).astype(bf16)
    return jnp.dot(high, matrix, preferred_element_type=f32) + jnp.dot(
        low, matrix, preferred_element_type=f32
    )


def head_mean(x, head_width):
    same = iota((LANES, LANES), 0) // head_width == iota((LANES, LANES), 1) // head_width
    return split_dot(x, jnp.where(same, 1.0 / head_width, 0.0).astype(bf16))


def unit_and_scale(rows, head_width):
    widened = rows.astype(f32)
    scale = lax.rsqrt(head_mean(widened * widened, head_width) + epsilon)
    return widened * scale, scale


def norm_backward(grad_hat, unit, scale, gain, head_width):
    grad_unit = grad_hat * gain
    inner = head_mean(grad_unit * unit, head_width)
    return scale * (grad_unit - unit * inner)


def rows8(x):
    return jnp.sum(x.reshape(x.shape[0] // 8, 8, x.shape[1]), axis=0)


def both_heads(gain_ref):
    gain = gain_ref[...]
    return jnp.concatenate([gain] * (LANES // gain.shape[1]), axis=1)


def each_pair(pairs, body):
    for p in range(pairs):
        body(p)


def at(tile):
    return pl.ds(tile * TILE, TILE)


def masks():
    key_pos = iota((TILE, WIDE), 0)
    query_pos = iota((TILE, WIDE), 1) % TILE
    return query_pos >= key_pos, key_pos // SEG >= query_pos // SEG


def as_column(row, rows):
    turned = jnp.broadcast_to(row, (LANES, rows)).T
    return turned


def own_kernel(
    q_hbm, k_hbm, v_hbm, g_hbm, q_gain_hbm, k_gain_hbm, table_hbm,
    qs_ref, gs_ref, kt_ref, qu_ref, e_ref, d32_ref, sum_ref, weighted_ref,
    bias_ref, gains_ref, kh_ref, q_ref, k_ref, v_ref, g_ref, q_gain_ref, k_gain_ref, table_ref, sems,
):
    sources = (q_gain_hbm, k_gain_hbm, table_hbm, k_hbm, q_hbm, g_hbm, v_hbm)
    targets = (q_gain_ref, k_gain_ref, table_ref, k_ref, q_ref, g_ref, v_ref)
    copies = [
        pltpu.make_async_copy(source, target, sems.at[i])
        for i, (source, target) in enumerate(zip(sources, targets))
    ]
    for copy in copies:
        copy.start()
    for copy in copies:
        copy.wait()
    rows = q_ref.shape[0]
    tiles = rows // TILE
    head_width = q_gain_ref.shape[1]
    q_gain, k_gain = both_heads(q_gain_ref), both_heads(k_gain_ref)
    gains_ref[...] = jnp.concatenate([q_gain, k_gain, jnp.zeros((6, LANES), f32)], axis=0)
    causal, _ = masks()
    first = iota((TILE, LANES), 1) < head_width
    zero = jnp.zeros((TILE, LANES), bf16)
    table = table_ref[...]
    near = table[:, :CLIP] - table[:, CLIP:]

    def body(p):
        lanes = pl.ds(p * LANES, LANES)
        unit, _ = unit_and_scale(k_ref[:, lanes], head_width)
        hat = (unit * k_gain).astype(bf16)
        kh_ref[p] = hat
        kt_ref[p] = hat.T
        unit, _ = unit_and_scale(q_ref[:, lanes], head_width)
        qu_ref[p] = unit
        hat = (unit * q_gain).astype(bf16) * jnp.asarray(head_width ** (-0.5), bf16)
        for b in range(tiles):
            part = hat[b * TILE : (b + 1) * TILE, :]
            grad = g_ref[at(b), lanes]
            qs_ref[p, pl.ds(b * WIDE, TILE), :] = jnp.where(first, part, zero)
            qs_ref[p, pl.ds(b * WIDE + TILE, TILE), :] = jnp.where(first, zero, part)
            gs_ref[p, pl.ds(b * WIDE, TILE), :] = jnp.where(first, grad, zero)
            gs_ref[p, pl.ds(b * WIDE + TILE, TILE), :] = jnp.where(first, zero, grad)
        skewed = [
            pltpu.roll(
                jnp.broadcast_to(near[2 * p + h : 2 * p + h + 1, :], (TILE, TILE)),
                0,
                1,
                stride=1,
                stride_axis=0,
            )
            for h in range(2)
        ]
        bias = jnp.concatenate(skewed, axis=1)
        below = jnp.where(causal, 0.0, bias)
        bias_ref[p] = below
        for b in range(tiles):
            queries = pl.ds(b * WIDE, WIDE)
            q_tile, g_tile = qs_ref[p, queries, :], gs_ref[p, queries, :]
            total = jnp.zeros((8, WIDE), f32)
            weighted = jnp.zeros((8, WIDE), f32)
            for a in range(b + 1):
                scores = lax.dot_general(
                    kh_ref[p, at(a), :], q_tile, ROWS_COLS, preferred_element_type=f32
                )
                if a == b:
                    scores = scores + bias
                if a == b - 1:
                    scores = scores + below
                e = jnp.exp(scores)
                if a == b:
                    e = jnp.where(causal, e, 0.0)
                d = lax.dot_general(
                    v_ref[at(a), lanes], g_tile, ROWS_COLS, preferred_element_type=f32
                )
                total = total + rows8(e)
                weighted = weighted + rows8(e * d)
                e_ref[p, at(a), queries] = e.astype(bf16)
                d32_ref[p, at(a), queries] = d
            sum_ref[p, :, queries] = total
            weighted_ref[p, :, queries] = weighted

    each_pair(qs_ref.shape[0], body)


def before_kernel(
    has_before, kr_ref, gains_ref, qs_ref, gs_ref, kt_ref, e_ref, sum_ref, bias_ref,
    kts_ref, er32_ref, er_ref, norm_ref, qn_ref, dv_ref, dvr_ref, krh_ref, gn_ref,
):
    rows, width = kr_ref.shape
    tiles = rows // TILE
    head_width = width // (2 * qs_ref.shape[0])
    before = has_before[0].astype(f32)
    k_gain = gains_ref[1:2, :]
    _, inside = masks()

    def body(p):
        lanes = pl.ds(p * LANES, LANES)
        unit, _ = unit_and_scale(kr_ref[:, lanes], head_width)
        hat = (unit * k_gain).astype(bf16)
        krh_ref[p] = hat
        kts_ref[p, :, :rows] = hat.T
        kts_ref[p, :, rows:] = kt_ref[p]
        for b in range(tiles):
            queries = pl.ds(b * WIDE, WIDE)
            q_tile = qs_ref[p, queries, :]
            total = jnp.zeros((8, WIDE), f32)
            for a in range(b, tiles):
                scores = lax.dot_general(
                    krh_ref[p, at(a), :], q_tile, ROWS_COLS, preferred_element_type=f32
                )
                if b == 0 and a == tiles - 1:
                    scores = scores + bias_ref[p]
                e = jnp.exp(scores)
                if a == b:
                    e = jnp.where(inside, e, 0.0)
                total = total + rows8(e)
                er_ref[p, at(a), queries] = e.astype(bf16)
                er32_ref[p, at(a), queries] = e
            normalizer = jnp.sum(
                sum_ref[p, :, queries] + total * before, axis=0, keepdims=True
            )
            norm_ref[p, :, queries] = jnp.broadcast_to(normalizer, (8, WIDE))
            column = as_column(1.0 / normalizer, WIDE)
            qn_ref[p, queries, :] = (q_tile.astype(f32) * column).astype(bf16)
            gn_ref[queries, :] = (gs_ref[p, queries, :].astype(f32) * column).astype(bf16)
        for a in range(tiles):
            span = pl.ds(0, (a + 1) * WIDE)
            dvr_ref[at(a), lanes] = jnp.dot(
                er_ref[p, at(a), span], gn_ref[span, :], preferred_element_type=f32
            ).astype(bf16)
        for a in range(tiles):
            span = pl.ds(a * WIDE, (tiles - a) * WIDE)
            dv_ref[at(a), lanes] = jnp.dot(
                e_ref[p, at(a), span], gn_ref[span, :], preferred_element_type=f32
            )

    each_pair(qs_ref.shape[0], body)


def grad_kernel(
    has_before, vr_ref, dd_ref, gs_ref, qn_ref, kts_ref, qu_ref, e_ref, er_ref, el_ref, norm_ref,
    weighted_ref,
    dq_ref, dk_ref, dkr_ref, stats_hbm, s_ref, d_ref, delta_ref, table_ref, sem,
):
    rows, width = vr_ref.shape
    tiles = rows // TILE
    pairs = qn_ref.shape[0]
    heads = 2 * pairs
    head_width = width // heads
    before = has_before[0].astype(f32)
    causal, _ = masks()
    one_lane = iota((1, LANES), 1)
    always = has_before[0] > -1
    still = has_before[0] > -2

    @pl.when(always)
    def _():
        for p in range(pairs):
            lanes = pl.ds(p * LANES, LANES)
            for b in range(tiles):
                queries = pl.ds(b * WIDE, WIDE)
                g_tile = gs_ref[p, queries, :]
                weighted = weighted_ref[p, :, queries]
                for a in range(b, tiles):
                    d = lax.dot_general(
                        vr_ref[at(a), lanes], g_tile, ROWS_COLS, preferred_element_type=f32
                    )
                    d_ref[p, at(a), queries] = d
                    weighted = weighted + rows8(er_ref[p, at(a), queries] * d)
                weighted = jnp.sum(weighted, axis=0, keepdims=True)
                normalizer = norm_ref[p, 0:1, queries]
                inverse = 1.0 / normalizer
                delta = weighted * inverse
                rest = (weighted - delta * normalizer) * inverse
                delta_ref[p, :, queries] = jnp.concatenate([inverse, delta, rest], axis=0)

    @pl.when(still)
    def _():
        for p in range(pairs):
            lanes = pl.ds(p * LANES, LANES)
            for b in range(tiles):
                queries = pl.ds(b * WIDE, WIDE)
                delta = delta_ref[p, 1:2, queries]
                for a in range(b, tiles):
                    s = (d_ref[p, at(a), queries] - delta).astype(bf16)
                    s_ref[p, at(a), queries] = el_ref[p, at(a), queries] * s
                for a in range(b + 1):
                    s = (dd_ref[p, at(a), queries] - delta).astype(bf16)
                    s_ref[p, at(tiles + a), queries] = e_ref[p, at(a), queries] * s

    @pl.when(still)
    def _():
        for p in range(pairs):
            for b in range(tiles):
                queries = pl.ds(b * WIDE, WIDE)
                span = pl.ds(b * TILE, rows + TILE)
                turned = jnp.dot(
                    kts_ref[p, :, span], s_ref[p, span, queries], preferred_element_type=f32
                )
                turned = jnp.concatenate(
                    [turned[:head_width, :TILE], turned[head_width:, TILE:]], axis=0
                )
                inverse = delta_ref[p, 0:1, queries] * head_width ** (-0.5)
                inverse = jnp.concatenate(
                    [
                        jnp.broadcast_to(inverse[:, :TILE], (head_width, TILE)),
                        jnp.broadcast_to(inverse[:, TILE:], (head_width, TILE)),
                    ],
                    axis=0,
                )
                dq_ref[p, at(b), :] = (turned * inverse).T

    def key_gradients(p, key_tiles):
        lanes = pl.ds(p * LANES, LANES)
        for a in key_tiles:
            low, high = max(0, a - tiles), min(tiles - 1, a)
            span = pl.ds(low * WIDE, (high - low + 1) * WIDE)
            dk = jnp.dot(s_ref[p, at(a), span], qn_ref[p, span, :], preferred_element_type=f32)
            if a < tiles:
                dkr_ref[at(a), lanes] = dk.astype(bf16)
            else:
                dk_ref[p, at(a - tiles), :] = dk

    @pl.when(still)
    def _():
        q_sum = jnp.zeros((8, LANES), f32)
        for p in range(pairs):
            q_sum = q_sum + rows8(dq_ref[p] * qu_ref[p])
        q_sum = jnp.sum(q_sum, axis=0, keepdims=True)
        flip = iota((TILE, TILE), 0) + iota((TILE, TILE), 1) == TILE - 1
        flip = jnp.where(flip, 1.0, 0.0).astype(bf16)
        lines = []
        last = jnp.zeros((1, LANES), f32)
        for p in range(pairs):
            near_grad = jnp.zeros((TILE, WIDE), f32)
            total = jnp.zeros((1, WIDE), f32)
            for b in range(tiles):
                queries = pl.ds(b * WIDE, WIDE)
                total = total + delta_ref[p, 2:3, queries]
                below = s_ref[p, at(tiles + b - 1), queries]
                if b == 0:
                    below = below * before.astype(bf16)
                both = jnp.where(causal, s_ref[p, at(tiles + b), queries], below)
                near_grad = near_grad + both.astype(f32) * delta_ref[p, 0:1, queries]
            near_grad = split_dot_left(flip, near_grad)
            for h in range(2):
                half = slice(h * TILE, (h + 1) * TILE)
                straight = pltpu.roll(near_grad[:, half], 1, 1, stride=1, stride_axis=0)
                taps = jnp.sum(straight, axis=0, keepdims=True)
                lines.append(taps)
                rest = jnp.sum(total[:, half] - taps, axis=1, keepdims=True)
                last = last + jnp.where(one_lane == 2 * p + h, rest, 0.0)
        lines += high_and_low(q_sum + pltpu.roll(q_sum, head_width, 1))
        lines += high_and_low(last)
        empty = table_ref.shape[1] - len(lines)
        if empty:
            lines.append(jnp.zeros((empty, LANES), f32))
        key_gradients(0, range(tiles))
        table = jnp.concatenate(lines, axis=0).astype(bf16)
        table_ref[...] = jnp.broadcast_to(table[None], table_ref.shape)

    copy = pltpu.make_async_copy(table_ref, stats_hbm, sem)
    copy.start()
    key_gradients(0, range(tiles, 2 * tiles))
    for p in range(1, pairs):
        key_gradients(p, range(2 * tiles))
    copy.wait()


def high_and_low(x):
    high = x.astype(bf16).astype(f32)
    return [high, x - high]


def split_dot_left(matrix, x):
    high = x.astype(bf16)
    low = (x - high.astype(f32)).astype(bf16)
    return jnp.dot(matrix, high, preferred_element_type=f32) + jnp.dot(
        matrix, low, preferred_element_type=f32
    )


def finish_kernel(
    gains_ref, dqh_ref, q_ref, k_ref, dk_ref, dv_ref, dkb_ref, dvb_ref, dq_out, dk_out, dv_out
):
    pairs = dqh_ref.shape[0]
    head_width = k_ref.shape[1] // (2 * pairs)
    q_gain, k_gain = gains_ref[0:1, :], gains_ref[1:2, :]

    def body(p):
        lanes = pl.ds(p * LANES, LANES)
        unit, scale = unit_and_scale(q_ref[:, lanes], head_width)
        dq_out[:, lanes] = norm_backward(dqh_ref[p], unit, scale, q_gain, head_width).astype(bf16)
        unit, scale = unit_and_scale(k_ref[:, lanes], head_width)
        grad_hat = dk_ref[p] + dkb_ref[:, lanes].astype(f32)
        dk_out[:, lanes] = norm_backward(grad_hat, unit, scale, k_gain, head_width).astype(bf16)
        dv_out[:, lanes] = (dv_ref[:, lanes] + dvb_ref[:, lanes].astype(f32)).astype(bf16)

    each_pair(pairs, body)


def total_kernel(tp_index, gains_ref, all_ref, q_gain_out, k_gain_out, bias_out):
    heads = bias_out.shape[0]
    head_width = q_gain_out.shape[1]
    everyone = jnp.sum(all_ref[...].astype(f32), axis=0)
    gains = jnp.sum(everyone[:, heads : heads + 2, :], axis=0)
    gains = gains[0:1, :] + gains[1:2, :]
    q_gain_out[...] = gains[:, :head_width]
    ratio = gains_ref[0:1, :head_width] / gains_ref[1:2, :head_width]
    k_gain_out[...] = gains[:, :head_width] * ratio
    mine = iota(everyone.shape, 0) == tp_index[0]
    summed = jnp.sum(jnp.where(mine, everyone, 0.0), axis=0)
    bias_out[:, :CLIP] = summed[:heads, :]
    last = summed[heads + 2 : heads + 3, :] + summed[heads + 3 : heads + 4, :]
    diagonal = iota((heads, LANES), 0) == iota((heads, LANES), 1)
    bias_out[:, CLIP:] = jnp.sum(jnp.where(diagonal, last, 0.0), axis=1, keepdims=True)


def call(kernel, args, outs, scratch=(), scalars=0, hbm=0, out_hbm=(), flops=0):
    args = [
        pltpu.with_memory_space_constraint(x, pltpu.HBM) if scalars <= i < scalars + hbm else x
        for i, x in enumerate(args)
    ]
    specs = [pl.BlockSpec(memory_space=pltpu.SMEM)] * scalars
    specs += [pl.BlockSpec(memory_space=pltpu.HBM)] * hbm
    specs += [pl.BlockSpec(memory_space=pltpu.VMEM)] * (len(args) - scalars - hbm)
    return pl.pallas_call(
        kernel,
        in_specs=specs,
        out_specs=[
            pl.BlockSpec(memory_space=pltpu.HBM if i in out_hbm else pltpu.VMEM)
            for i in range(len(outs))
        ],
        out_shape=[jax.ShapeDtypeStruct(*o) for o in outs],
        scratch_shapes=list(scratch),
        compiler_params=pltpu.CompilerParams(vmem_limit_bytes=GRANT),
        cost_estimate=pl.CostEstimate(flops=flops, bytes_accessed=0, transcendentals=0),
    )(*args)


def per_device(query, key, value, out_grad, query_gain, key_gain, rel_bias):
    rows, width = query.shape
    heads = rel_bias.shape[0]
    head_width = width // heads
    pairs = width // LANES
    double = 2 * rows
    before_key = shifted(key, "sp", 1)
    before_value = shifted(value, "sp", 1)
    q_gain, k_gain = query_gain[None, :], key_gain[None, :]
    has_before = (lax.axis_index("sp") > 0).astype(jnp.int32).reshape(1)
    tp_index = lax.axis_index("tp").astype(jnp.int32).reshape(1)
    stacked = ((pairs, double, LANES), bf16)
    hats = ((pairs, rows, LANES), bf16)
    turned = ((pairs, LANES, rows), bf16)
    units = ((pairs, rows, LANES), f32)
    square = ((pairs, rows, double), bf16)
    square32 = ((pairs, rows, double), f32)
    line = ((pairs, 8, double), f32)
    flat, flat_low = ((rows, width), f32), ((rows, width), bf16)
    gains = ((8, LANES), f32)
    qs, gs, kt, qu, e, d32, sums, weighted, bias, gains = call(
        own_kernel,
        (query, key, value, out_grad, q_gain, k_gain, rel_bias),
        (stacked, stacked, turned, units, square, square32, line, line,
         ((pairs, TILE, WIDE), f32), gains),
        scratch=[pltpu.VMEM(*hats)]
        + [pltpu.VMEM(*flat_low)] * 4
        + [pltpu.VMEM(q_gain.shape, f32), pltpu.VMEM(k_gain.shape, f32)]
        + [pltpu.VMEM(rel_bias.shape, f32), pltpu.SemaphoreType.DMA((7,))],
        hbm=7,
        flops=4_000_000_000,
    )
    kts, er32, er, norm, qn, dv, dv_before = call(
        before_kernel,
        (has_before, before_key, gains, qs, gs, kt, e, sums, bias),
        (((pairs, LANES, double), bf16), square32, square, line, stacked, flat, flat_low),
        scratch=[pltpu.VMEM(*hats), pltpu.VMEM((double, LANES), bf16)],
        scalars=1,
        flops=4_000_000_000,
    )
    dv_back = shifted(dv_before, "sp", -1)
    stat_rows = -(-(heads + 4) // 8) * 8
    members = (lax.axis_size("sp"), lax.axis_size("tp"))
    spread = ((members[0] * members[1], stat_rows, LANES), bf16)
    dq_hat, dk, dk_before, stats = call(
        grad_kernel,
        (has_before, before_value, d32, gs, qn, kts, qu, e, er32, er, norm, weighted),
        (units, units, flat_low, spread),
        out_hbm=(3,),
        scratch=[pltpu.VMEM((pairs, double, double), bf16), pltpu.VMEM(*square32)]
        + [pltpu.VMEM((pairs, 3, double), f32), pltpu.VMEM(*spread), pltpu.SemaphoreType.DMA],
        scalars=1,
        flops=8_000_000_000,
    )
    dk_back = shifted(dk_before, "sp", -1)
    everyone = lax.all_to_all(stats, ("sp", "tp"), 0, 0, tiled=True)
    everyone = everyone.reshape(members + (stat_rows, LANES))
    dq, dk, dv = call(
        finish_kernel,
        (gains, dq_hat, query, key, dk, dv, dk_back, dv_back),
        (flat_low, flat_low, flat_low),
        flops=1_000_000_000,
    )
    q_gain_grad, k_gain_grad, bias_grad = call(
        total_kernel,
        (tp_index, gains, everyone),
        (((1, head_width), f32), ((1, head_width), f32), ((heads, CLIP + 1), f32)),
        scalars=1,
        flops=1_000_000,
    )
    return (dq, dk, dv, q_gain_grad[0], k_gain_grad[0], bias_grad)


def solution(mesh):
    placed = (P("sp", "tp"), P("sp", "tp"), P("sp", "tp"), P("sp", "tp"), P(), P(), P("tp", None))
    return jax.shard_map(
        per_device,
        mesh=mesh,
        in_specs=placed,
        out_specs=(P("sp", "tp"), P("sp", "tp"), P("sp", "tp"), P(), P(), P("tp", None)),
        check_vma=False,
    )
```

```python
import jax
import jax.numpy as jnp
from jax import lax
from jax.experimental import pallas as pl
from jax.experimental.pallas import tpu as pltpu
from jax.sharding import PartitionSpec as P


SEG = 64
CLIP = 128
LANES = 128
TILE = 128
WIDE = 2 * TILE
GRANT = 16 * 1024 * 1024

epsilon = 1e-06
f32 = jnp.float32
bf16 = jnp.bfloat16

ROWS_COLS = (((1,), (1,)), ((), ()))


def shifted(block, axis, distance):
    devices = range(lax.axis_size(axis))
    route = [(i - distance, i) for i in devices if i - distance in devices]
    return lax.ppermute(block, axis, route)


def iota(shape, dim):
    return lax.broadcasted_iota(jnp.int32, shape, dim)


def split_dot(x, matrix):
    high = x.astype(bf16)
    low = (x - high.astype(f32)).astype(bf16)
    return jnp.dot(high, matrix, preferred_element_type=f32) + jnp.dot(
        low, matrix, preferred_element_type=f32
    )


def head_mean(x, head_width):
    same = iota((LANES, LANES), 0) // head_width == iota((LANES, LANES), 1) // head_width
    return split_dot(x, jnp.where(same, 1.0 / head_width, 0.0).astype(bf16))


def unit_and_scale(rows, head_width):
    widened = rows.astype(f32)
    scale = lax.rsqrt(head_mean(widened * widened, head_width) + epsilon)
    return widened * scale, scale


def norm_backward(grad_hat, unit, scale, gain, head_width):
    grad_unit = grad_hat * gain
    inner = head_mean(grad_unit * unit, head_width)
    return scale * (grad_unit - unit * inner)


def rows8(x):
    return jnp.sum(x.reshape(x.shape[0] // 8, 8, x.shape[1]), axis=0)


def both_heads(gain_ref):
    gain = gain_ref[...]
    return jnp.concatenate([gain] * (LANES // gain.shape[1]), axis=1)


def each_pair(pairs, body):
    for p in range(pairs):
        body(p)


def at(tile):
    return pl.ds(tile * TILE, TILE)


def masks():
    key_pos = iota((TILE, WIDE), 0)
    query_pos = iota((TILE, WIDE), 1) % TILE
    return query_pos >= key_pos, key_pos // SEG >= query_pos // SEG


def as_column(row, rows):
    turned = jnp.broadcast_to(row, (LANES, rows)).T
    return turned


def own_kernel(
    q_hbm, k_hbm, v_hbm, g_hbm, q_gain_hbm, k_gain_hbm, table_hbm,
    qs_ref, gs_ref, kt_ref, qu_ref, e_ref, e32_ref, d32_ref, sum_ref, weighted_ref,
    bias_ref, gains_ref, kh_ref, q_ref, k_ref, v_ref, g_ref, q_gain_ref, k_gain_ref, table_ref, sems,
):
    sources = (q_gain_hbm, k_gain_hbm, table_hbm, k_hbm, q_hbm, g_hbm, v_hbm)
    targets = (q_gain_ref, k_gain_ref, table_ref, k_ref, q_ref, g_ref, v_ref)
    copies = [
        pltpu.make_async_copy(source, target, sems.at[i])
        for i, (source, target) in enumerate(zip(sources, targets))
    ]
    for copy in copies:
        copy.start()
    for copy in copies:
        copy.wait()
    rows = q_ref.shape[0]
    tiles = rows // TILE
    head_width = q_gain_ref.shape[1]
    q_gain, k_gain = both_heads(q_gain_ref), both_heads(k_gain_ref)
    gains_ref[...] = jnp.concatenate([q_gain, k_gain, jnp.zeros((6, LANES), f32)], axis=0)
    causal, _ = masks()
    first = iota((TILE, LANES), 1) < head_width
    zero = jnp.zeros((TILE, LANES), bf16)
    table = table_ref[...]
    near = table[:, :CLIP] - table[:, CLIP:]

    def body(p):
        lanes = pl.ds(p * LANES, LANES)
        unit, _ = unit_and_scale(k_ref[:, lanes], head_width)
        hat = (unit * k_gain).astype(bf16)
        kh_ref[p] = hat
        kt_ref[p] = hat.T
        unit, _ = unit_and_scale(q_ref[:, lanes], head_width)
        qu_ref[p] = unit
        hat = (unit * q_gain).astype(bf16) * jnp.asarray(head_width ** (-0.5), bf16)
        for b in range(tiles):
            part = hat[b * TILE : (b + 1) * TILE, :]
            grad = g_ref[at(b), lanes]
            qs_ref[p, pl.ds(b * WIDE, TILE), :] = jnp.where(first, part, zero)
            qs_ref[p, pl.ds(b * WIDE + TILE, TILE), :] = jnp.where(first, zero, part)
            gs_ref[p, pl.ds(b * WIDE, TILE), :] = jnp.where(first, grad, zero)
            gs_ref[p, pl.ds(b * WIDE + TILE, TILE), :] = jnp.where(first, zero, grad)
        skewed = [
            pltpu.roll(
                jnp.broadcast_to(near[2 * p + h : 2 * p + h + 1, :], (TILE, TILE)),
                0,
                1,
                stride=1,
                stride_axis=0,
            )
            for h in range(2)
        ]
        bias = jnp.concatenate(skewed, axis=1)
        below = jnp.where(causal, 0.0, bias)
        bias_ref[p] = below
        for b in range(tiles):
            queries = pl.ds(b * WIDE, WIDE)
            q_tile, g_tile = qs_ref[p, queries, :], gs_ref[p, queries, :]
            total = jnp.zeros((8, WIDE), f32)
            weighted = jnp.zeros((8, WIDE), f32)
            for a in range(b + 1):
                scores = lax.dot_general(
                    kh_ref[p, at(a), :], q_tile, ROWS_COLS, preferred_element_type=f32
                )
                if a == b:
                    scores = scores + bias
                if a == b - 1:
                    scores = scores + below
                e = jnp.exp(scores)
                if a == b:
                    e = jnp.where(causal, e, 0.0)
                d = lax.dot_general(
                    v_ref[at(a), lanes], g_tile, ROWS_COLS, preferred_element_type=f32
                )
                total = total + rows8(e)
                weighted = weighted + rows8(e * d)
                e_ref[p, at(a), queries] = e.astype(bf16)
                e32_ref[p, at(a), queries] = e
                d32_ref[p, at(a), queries] = d
            sum_ref[p, :, queries] = total
            weighted_ref[p, :, queries] = weighted

    each_pair(qs_ref.shape[0], body)


def before_kernel(
    has_before, kr_ref, gains_ref, qs_ref, gs_ref, kt_ref, e_ref, sum_ref, bias_ref,
    kts_ref, er32_ref, norm_ref, qn_ref, dv_ref, dvr_ref, krh_ref, gn_ref, er_ref,
):
    rows, width = kr_ref.shape
    tiles = rows // TILE
    head_width = width // (2 * qs_ref.shape[0])
    before = has_before[0].astype(f32)
    k_gain = gains_ref[1:2, :]
    _, inside = masks()

    def body(p):
        lanes = pl.ds(p * LANES, LANES)
        unit, _ = unit_and_scale(kr_ref[:, lanes], head_width)
        hat = (unit * k_gain).astype(bf16)
        krh_ref[p] = hat
        kts_ref[p, :, :rows] = hat.T
        kts_ref[p, :, rows:] = kt_ref[p]
        for b in range(tiles):
            queries = pl.ds(b * WIDE, WIDE)
            q_tile = qs_ref[p, queries, :]
            total = jnp.zeros((8, WIDE), f32)
            for a in range(b, tiles):
                scores = lax.dot_general(
                    krh_ref[p, at(a), :], q_tile, ROWS_COLS, preferred_element_type=f32
                )
                if b == 0 and a == tiles - 1:
                    scores = scores + bias_ref[p]
                e = jnp.exp(scores)
                if a == b:
                    e = jnp.where(inside, e, 0.0)
                total = total + rows8(e)
                er_ref[p, at(a), queries] = e.astype(bf16)
                er32_ref[p, at(a), queries] = e
            normalizer = jnp.sum(
                sum_ref[p, :, queries] + total * before, axis=0, keepdims=True
            )
            norm_ref[p, :, queries] = jnp.broadcast_to(normalizer, (8, WIDE))
            column = as_column(1.0 / normalizer, WIDE)
            qn_ref[p, queries, :] = (q_tile.astype(f32) * column).astype(bf16)
            gn_ref[queries, :] = (gs_ref[p, queries, :].astype(f32) * column).astype(bf16)
        for a in range(tiles):
            span = pl.ds(0, (a + 1) * WIDE)
            dvr_ref[at(a), lanes] = jnp.dot(
                er_ref[p, at(a), span], gn_ref[span, :], preferred_element_type=f32
            ).astype(bf16)
        for a in range(tiles):
            span = pl.ds(a * WIDE, (tiles - a) * WIDE)
            dv_ref[at(a), lanes] = jnp.dot(
                e_ref[p, at(a), span], gn_ref[span, :], preferred_element_type=f32
            )

    each_pair(qs_ref.shape[0], body)


def grad_kernel(
    has_before, vr_ref, dd_ref, gs_ref, qn_ref, kts_ref, qu_ref, e_ref, er_ref, norm_ref,
    weighted_ref,
    dq_ref, dk_ref, dkr_ref, stats_hbm, s_ref, d_ref, delta_ref, table_ref, sem,
):
    rows, width = vr_ref.shape
    tiles = rows // TILE
    pairs = qn_ref.shape[0]
    heads = 2 * pairs
    head_width = width // heads
    before = has_before[0].astype(f32)
    causal, _ = masks()
    one_lane = iota((1, LANES), 1)
    always = has_before[0] > -1
    still = has_before[0] > -2

    @pl.when(always)
    def _():
        for p in range(pairs):
            lanes = pl.ds(p * LANES, LANES)
            for b in range(tiles):
                queries = pl.ds(b * WIDE, WIDE)
                g_tile = gs_ref[p, queries, :]
                weighted = weighted_ref[p, :, queries]
                for a in range(b, tiles):
                    d = lax.dot_general(
                        vr_ref[at(a), lanes], g_tile, ROWS_COLS, preferred_element_type=f32
                    )
                    d_ref[p, at(a), queries] = d
                    weighted = weighted + rows8(er_ref[p, at(a), queries] * d)
                weighted = jnp.sum(weighted, axis=0, keepdims=True)
                normalizer = norm_ref[p, 0:1, queries]
                inverse = 1.0 / normalizer
                delta = weighted * inverse
                rest = (weighted - delta * normalizer) * inverse
                delta_ref[p, :, queries] = jnp.concatenate([inverse, delta, rest], axis=0)

    @pl.when(still)
    def _():
        for p in range(pairs):
            lanes = pl.ds(p * LANES, LANES)
            for b in range(tiles):
                queries = pl.ds(b * WIDE, WIDE)
                delta = delta_ref[p, 1:2, queries]
                for a in range(b, tiles):
                    s = er_ref[p, at(a), queries] * (d_ref[p, at(a), queries] - delta)
                    s_ref[p, at(a), queries] = s.astype(bf16)
                for a in range(b + 1):
                    s = e_ref[p, at(a), queries] * (dd_ref[p, at(a), queries] - delta)
                    s_ref[p, at(tiles + a), queries] = s.astype(bf16)

    @pl.when(still)
    def _():
        for p in range(pairs):
            for b in range(tiles):
                queries = pl.ds(b * WIDE, WIDE)
                span = pl.ds(b * TILE, rows + TILE)
                turned = jnp.dot(
                    kts_ref[p, :, span], s_ref[p, span, queries], preferred_element_type=f32
                )
                turned = jnp.concatenate(
                    [turned[:head_width, :TILE], turned[head_width:, TILE:]], axis=0
                )
                inverse = delta_ref[p, 0:1, queries] * head_width ** (-0.5)
                inverse = jnp.concatenate(
                    [
                        jnp.broadcast_to(inverse[:, :TILE], (head_width, TILE)),
                        jnp.broadcast_to(inverse[:, TILE:], (head_width, TILE)),
                    ],
                    axis=0,
                )
                dq_ref[p, at(b), :] = (turned * inverse).T

    def key_gradients(p, key_tiles):
        lanes = pl.ds(p * LANES, LANES)
        for a in key_tiles:
            low, high = max(0, a - tiles), min(tiles - 1, a)
            span = pl.ds(low * WIDE, (high - low + 1) * WIDE)
            dk = jnp.dot(s_ref[p, at(a), span], qn_ref[p, span, :], preferred_element_type=f32)
            if a < tiles:
                dkr_ref[at(a), lanes] = dk.astype(bf16)
            else:
                dk_ref[p, at(a - tiles), :] = dk

    @pl.when(still)
    def _():
        q_sum = jnp.zeros((8, LANES), f32)
        for p in range(pairs):
            q_sum = q_sum + rows8(dq_ref[p] * qu_ref[p])
        q_sum = jnp.sum(q_sum, axis=0, keepdims=True)
        flip = iota((TILE, TILE), 0) + iota((TILE, TILE), 1) == TILE - 1
        flip = jnp.where(flip, 1.0, 0.0).astype(bf16)
        lines = []
        last = jnp.zeros((1, LANES), f32)
        for p in range(pairs):
            near_grad = jnp.zeros((TILE, WIDE), f32)
            total = jnp.zeros((1, WIDE), f32)
            for b in range(tiles):
                queries = pl.ds(b * WIDE, WIDE)
                total = total + delta_ref[p, 2:3, queries]
                below = s_ref[p, at(tiles + b - 1), queries]
                if b == 0:
                    below = below * before.astype(bf16)
                both = jnp.where(causal, s_ref[p, at(tiles + b), queries], below)
                near_grad = near_grad + both.astype(f32) * delta_ref[p, 0:1, queries]
            near_grad = split_dot_left(flip, near_grad)
            for h in range(2):
                half = slice(h * TILE, (h + 1) * TILE)
                straight = pltpu.roll(near_grad[:, half], 1, 1, stride=1, stride_axis=0)
                taps = jnp.sum(straight, axis=0, keepdims=True)
                lines.append(taps)
                rest = jnp.sum(total[:, half] - taps, axis=1, keepdims=True)
                last = last + jnp.where(one_lane == 2 * p + h, rest, 0.0)
        lines += high_and_low(q_sum + pltpu.roll(q_sum, head_width, 1))
        lines += high_and_low(last)
        empty = table_ref.shape[1] - len(lines)
        if empty:
            lines.append(jnp.zeros((empty, LANES), f32))
        key_gradients(0, range(tiles))
        table = jnp.concatenate(lines, axis=0).astype(bf16)
        table_ref[...] = jnp.broadcast_to(table[None], table_ref.shape)

    copy = pltpu.make_async_copy(table_ref, stats_hbm, sem)
    copy.start()
    key_gradients(0, range(tiles, 2 * tiles))
    for p in range(1, pairs):
        key_gradients(p, range(2 * tiles))
    copy.wait()


def high_and_low(x):
    high = x.astype(bf16).astype(f32)
    return [high, x - high]


def split_dot_left(matrix, x):
    high = x.astype(bf16)
    low = (x - high.astype(f32)).astype(bf16)
    return jnp.dot(matrix, high, preferred_element_type=f32) + jnp.dot(
        matrix, low, preferred_element_type=f32
    )


def finish_kernel(
    gains_ref, dqh_ref, q_ref, k_ref, dk_ref, dv_ref, dkb_ref, dvb_ref, dq_out, dk_out, dv_out
):
    pairs = dqh_ref.shape[0]
    head_width = k_ref.shape[1] // (2 * pairs)
    q_gain, k_gain = gains_ref[0:1, :], gains_ref[1:2, :]

    def body(p):
        lanes = pl.ds(p * LANES, LANES)
        unit, scale = unit_and_scale(q_ref[:, lanes], head_width)
        dq_out[:, lanes] = norm_backward(dqh_ref[p], unit, scale, q_gain, head_width).astype(bf16)
        unit, scale = unit_and_scale(k_ref[:, lanes], head_width)
        grad_hat = dk_ref[p] + dkb_ref[:, lanes].astype(f32)
        dk_out[:, lanes] = norm_backward(grad_hat, unit, scale, k_gain, head_width).astype(bf16)
        dv_out[:, lanes] = (dv_ref[:, lanes] + dvb_ref[:, lanes].astype(f32)).astype(bf16)

    each_pair(pairs, body)


def total_kernel(tp_index, gains_ref, all_ref, q_gain_out, k_gain_out, bias_out):
    heads = bias_out.shape[0]
    head_width = q_gain_out.shape[1]
    everyone = jnp.sum(all_ref[...].astype(f32), axis=0)
    gains = jnp.sum(everyone[:, heads : heads + 2, :], axis=0)
    gains = gains[0:1, :] + gains[1:2, :]
    q_gain_out[...] = gains[:, :head_width]
    ratio = gains_ref[0:1, :head_width] / gains_ref[1:2, :head_width]
    k_gain_out[...] = gains[:, :head_width] * ratio
    mine = iota(everyone.shape, 0) == tp_index[0]
    summed = jnp.sum(jnp.where(mine, everyone, 0.0), axis=0)
    bias_out[:, :CLIP] = summed[:heads, :]
    last = summed[heads + 2 : heads + 3, :] + summed[heads + 3 : heads + 4, :]
    diagonal = iota((heads, LANES), 0) == iota((heads, LANES), 1)
    bias_out[:, CLIP:] = jnp.sum(jnp.where(diagonal, last, 0.0), axis=1, keepdims=True)


def call(kernel, args, outs, scratch=(), scalars=0, hbm=0, out_hbm=(), flops=0):
    args = [
        pltpu.with_memory_space_constraint(x, pltpu.HBM) if scalars <= i < scalars + hbm else x
        for i, x in enumerate(args)
    ]
    specs = [pl.BlockSpec(memory_space=pltpu.SMEM)] * scalars
    specs += [pl.BlockSpec(memory_space=pltpu.HBM)] * hbm
    specs += [pl.BlockSpec(memory_space=pltpu.VMEM)] * (len(args) - scalars - hbm)
    return pl.pallas_call(
        kernel,
        in_specs=specs,
        out_specs=[
            pl.BlockSpec(memory_space=pltpu.HBM if i in out_hbm else pltpu.VMEM)
            for i in range(len(outs))
        ],
        out_shape=[jax.ShapeDtypeStruct(*o) for o in outs],
        scratch_shapes=list(scratch),
        compiler_params=pltpu.CompilerParams(vmem_limit_bytes=GRANT),
        cost_estimate=pl.CostEstimate(flops=flops, bytes_accessed=0, transcendentals=0),
    )(*args)


def per_device(query, key, value, out_grad, query_gain, key_gain, rel_bias):
    rows, width = query.shape
    heads = rel_bias.shape[0]
    head_width = width // heads
    pairs = width // LANES
    double = 2 * rows
    before_key = shifted(key, "sp", 1)
    before_value = shifted(value, "sp", 1)
    q_gain, k_gain = query_gain[None, :], key_gain[None, :]
    has_before = (lax.axis_index("sp") > 0).astype(jnp.int32).reshape(1)
    tp_index = lax.axis_index("tp").astype(jnp.int32).reshape(1)
    stacked = ((pairs, double, LANES), bf16)
    hats = ((pairs, rows, LANES), bf16)
    turned = ((pairs, LANES, rows), bf16)
    units = ((pairs, rows, LANES), f32)
    square = ((pairs, rows, double), bf16)
    square32 = ((pairs, rows, double), f32)
    line = ((pairs, 8, double), f32)
    flat, flat_low = ((rows, width), f32), ((rows, width), bf16)
    gains = ((8, LANES), f32)
    qs, gs, kt, qu, e, e32, d32, sums, weighted, bias, gains = call(
        own_kernel,
        (query, key, value, out_grad, q_gain, k_gain, rel_bias),
        (stacked, stacked, turned, units, square, square32, square32, line, line,
         ((pairs, TILE, WIDE), f32), gains),
        scratch=[pltpu.VMEM(*hats)]
        + [pltpu.VMEM(*flat_low)] * 4
        + [pltpu.VMEM(q_gain.shape, f32), pltpu.VMEM(k_gain.shape, f32)]
        + [pltpu.VMEM(rel_bias.shape, f32), pltpu.SemaphoreType.DMA((7,))],
        hbm=7,
        flops=4_000_000_000,
    )
    kts, er32, norm, qn, dv, dv_before = call(
        before_kernel,
        (has_before, before_key, gains, qs, gs, kt, e, sums, bias),
        (((pairs, LANES, double), bf16), square32, line, stacked, flat, flat_low),
        scratch=[pltpu.VMEM(*hats), pltpu.VMEM((double, LANES), bf16), pltpu.VMEM(*square)],
        scalars=1,
        flops=4_000_000_000,
    )
    dv_back = shifted(dv_before, "sp", -1)
    stat_rows = -(-(heads + 4) // 8) * 8
    members = (lax.axis_size("sp"), lax.axis_size("tp"))
    spread = ((members[0] * members[1], stat_rows, LANES), bf16)
    dq_hat, dk, dk_before, stats = call(
        grad_kernel,
        (has_before, before_value, d32, gs, qn, kts, qu, e32, er32, norm, weighted),
        (units, units, flat_low, spread),
        out_hbm=(3,),
        scratch=[pltpu.VMEM((pairs, double, double), bf16), pltpu.VMEM(*square32)]
        + [pltpu.VMEM((pairs, 3, double), f32), pltpu.VMEM(*spread), pltpu.SemaphoreType.DMA],
        scalars=1,
        flops=8_000_000_000,
    )
    dk_back = shifted(dk_before, "sp", -1)
    everyone = lax.all_to_all(stats, ("sp", "tp"), 0, 0, tiled=True)
    everyone = everyone.reshape(members + (stat_rows, LANES))
    dq, dk, dv = call(
        finish_kernel,
        (gains, dq_hat, query, key, dk, dv, dk_back, dv_back),
        (flat_low, flat_low, flat_low),
        flops=1_000_000_000,
    )
    q_gain_grad, k_gain_grad, bias_grad = call(
        total_kernel,
        (tp_index, gains, everyone),
        (((1, head_width), f32), ((1, head_width), f32), ((heads, CLIP + 1), f32)),
        scalars=1,
        flops=1_000_000,
    )
    return (dq, dk, dv, q_gain_grad[0], k_gain_grad[0], bias_grad)


def solution(mesh):
    placed = (P("sp", "tp"), P("sp", "tp"), P("sp", "tp"), P("sp", "tp"), P(), P(), P("tp", None))
    return jax.shard_map(
        per_device,
        mesh=mesh,
        in_specs=placed,
        out_specs=(P("sp", "tp"), P("sp", "tp"), P("sp", "tp"), P(), P(), P("tp", None)),
        check_vma=False,
    )
```
